32 devices in a mesh: sp: 8 (over z, x), tp: 4 (over y, core).
Axes of the slice: x: 2, y: 2, z: 4, core: 2. Of those that a mesh axis runs over, the one named last changes fastest.
Arguments:
- tokens: bfloat16 [4096, 2048], P('sp', 'tp'), may hold values from -72 to 72
- w_query: bfloat16 [2048, 1024], P('sp', 'tp'), may hold values from -0.125 to 0.125
- w_key: bfloat16 [2048, 256], P('sp', 'tp'), may hold values from -0.125 to 0.125
- w_value: bfloat16 [2048, 256], P('sp', 'tp'), may hold values from -0.125 to 0.125
- w_pool_in: bfloat16 [2048, 1024], P('sp', 'tp'), may hold values from -0.125 to 0.125
- sink: float32 [16], P('tp'), may hold values from 3 to 7
- w_pool: bfloat16 [4, 256, 256], P('tp'), may hold values from -0.375 to 0.375
- pool_scale: float32 [1024], P('tp'), may hold values from 0.1 to 1.9
- w_out_attn: bfloat16 [1024, 2048], P('tp', 'sp'), may hold values from -0.5 to 0.5
- w_out_pool: bfloat16 [1024, 2048], P('tp', 'sp'), may hold values from -0.125 to 0.125
- out_gain: float32 [2048], P('tp'), may hold values from 0.1 to 1.9
Outputs:
- mixed: bfloat16 [4096, 2048], P('sp', 'tp')
The draws below stay inside these ranges and needn't reach their ends.
All inputs are finite; a program needn't handle non-finite values.
Results may differ from the reference program's by a relative error of at most 0.012.
The reference program's roundings to bfloat16 on the way count: a program that leaves them out, or rounds other values in their place, can miss the bound.
Values may be sent and summed in bfloat16 or wider, within the bound.
No kernel may reach another device: no remote copies, remote signals or barrier semaphores. Data moves between devices by JAX's collectives and lax.ppermute only.
A program may use at most 64 MiB of HBM per device.

```python
import jax
import jax.numpy as jnp
from jax import lax

D = 2048
HEADS = 16
KV_HEADS = 4
HEAD_DIM = 64
POOL_GROUPS = 4
GROUP_DIM = 256
WINDOW = 128
SEQ = 4096
ATTN_WIDTH = 1024
KV_WIDTH = 256
POOL_WIDTH = 1024
N_TP = 4


def draw_tokens(key, part):
    base = jnp.clip(jax.random.normal(key, (SEQ, D), jnp.float32), -6.0, 6.0)
    return base.astype(jnp.bfloat16)


def levels(stream_key, dims, pieces, smallest, top_value):
    level = 1.0
    for position, shards_of in pieces:
        heights = jax.random.uniform(jax.random.fold_in(jax.random.fold_in(stream_key, 6), position), (shards_of,), jnp.float32, smallest / len(pieces), top_value / len(pieces))
        level = level * jnp.repeat(jnp.exp(heights), dims[position] // shards_of).reshape((-1,) + (1,) * (len(dims) - 1 - position))
    return level


def centred(rng, shape, deviation, bound, shards=(), kind=jnp.bfloat16):
    entries = jax.random.normal(rng, shape, jnp.float32) * deviation
    if len(shards) > 0:
        entries = levels(rng, shape, shards, -0.22, 0.18) * entries
    return jnp.clip(entries, min=-bound, max=bound).astype(kind)


def setup_inputs(seed: int = 0) -> dict:
    splits = jax.random.split(jax.random.key(seed), 12)
    return {
        "tokens": draw_tokens(jax.random.fold_in(splits[11], 71), 0),
        "w_query": centred(splits[1], (D, ATTN_WIDTH), D ** -0.5, 0.125, ((0, 8), (1, 4))),
        "w_key": centred(splits[2], (D, KV_WIDTH), D ** -0.5, 0.125, ((0, 8), (1, 4))),
        "w_value": centred(splits[3], (D, KV_WIDTH), D ** -0.5, 0.125, ((0, 8), (1, 4))),
        "w_pool_in": centred(splits[4], (D, POOL_WIDTH), D ** -0.5, 0.125, ((0, 8), (1, 4))),
        "sink": jnp.clip(3.0 + 4.0 * jax.random.uniform(splits[5], (HEADS,), jnp.float32) ** levels(splits[5], (HEADS,), ((0, 4),), -0.2, 0.2), 3.0, 7.0),
        "w_pool": centred(splits[6], (POOL_GROUPS, GROUP_DIM, GROUP_DIM), GROUP_DIM ** -0.5, 0.375, ((0, 4),)),
        "pool_scale": jnp.clip(1.0 + 0.18 * jax.random.normal(splits[7], (POOL_WIDTH,), jnp.float32), 0.1, 1.9),
        "w_out_attn": centred(splits[8], (ATTN_WIDTH, D), (ATTN_WIDTH // 8) ** -0.5, 0.5, ((0, 4), (1, 8))),
        "w_out_pool": centred(splits[9], (POOL_WIDTH, D), (ATTN_WIDTH + POOL_WIDTH) ** -0.5, 0.125, ((0, 4), (1, 8))),
        "out_gain": jnp.clip(1.0 + 0.18 * jax.random.normal(splits[10], (D,), jnp.float32), 0.1, 1.9),
    }


epsilon = 1e-05
masked_score = -1e+30

def attend_head(query_one, key_one, value_one, sink_one):
    seq_len = query_one.shape[0]
    group = query_one.shape[1]
    block_count = seq_len // WINDOW
    query_blocks = query_one.reshape(block_count, WINDOW, group, HEAD_DIM).astype(jnp.float32)

    def banded(source):
        padded = jnp.pad(source, ((WINDOW, WINDOW), (0, 0))).reshape(block_count + 2, WINDOW, HEAD_DIM)
        return jnp.concatenate([padded[:-2], padded[1:-1], padded[2:]], axis=1).astype(jnp.float32)
    key_band = banded(key_one)
    value_band = banded(value_one)
    scores = jnp.einsum('nqgd,nsd->ngqs', query_blocks, key_band) * HEAD_DIM ** (-0.5)
    starts = jnp.arange(block_count, dtype=jnp.int32) * WINDOW
    query_pos = starts[:, None] + jnp.arange(WINDOW, dtype=jnp.int32)[None, :]
    key_pos = starts[:, None] + jnp.arange(3 * WINDOW, dtype=jnp.int32)[None, :] - WINDOW
    distance = key_pos[:, None, :] - query_pos[:, :, None]
    inside = (key_pos >= 0) & (key_pos < seq_len)
    keep = (jnp.abs(distance) <= WINDOW) & inside[:, None, :]
    scores = jnp.where(keep[:, None], scores, masked_score)
    sink_logit = sink_one.astype(jnp.float32)[None, :, None, None]
    top = jnp.maximum(lax.optimization_barrier(jnp.max(scores, axis=-1, keepdims=True)), sink_logit)
    raised = jnp.exp(scores - top)
    total = lax.optimization_barrier(jnp.sum(raised, axis=-1, keepdims=True)) + jnp.exp(sink_logit - top)
    probs = (raised / total).astype(jnp.bfloat16)
    attended = jnp.einsum('ngqs,nsd->nqgd', probs.astype(jnp.float32), value_band)
    return attended.astype(jnp.bfloat16).reshape(seq_len, group * HEAD_DIM)

def reference(tokens, w_query, w_key, w_value, w_pool_in, sink, w_pool, pool_scale, w_out_attn, w_out_pool, out_gain):
    seq_len = tokens.shape[0]
    group = HEADS // KV_HEADS
    query = jnp.dot(tokens, w_query, preferred_element_type=jnp.float32).astype(jnp.bfloat16)
    keys = jnp.dot(tokens, w_key, preferred_element_type=jnp.float32).astype(jnp.bfloat16)
    values = jnp.dot(tokens, w_value, preferred_element_type=jnp.float32).astype(jnp.bfloat16)
    chan = jnp.dot(tokens, w_pool_in, preferred_element_type=jnp.float32).astype(jnp.bfloat16)
    query_heads = query.reshape(seq_len, KV_HEADS, group, HEAD_DIM).transpose(1, 0, 2, 3)
    key_heads = keys.reshape(seq_len, KV_HEADS, HEAD_DIM).transpose(1, 0, 2)
    value_heads = values.reshape(seq_len, KV_HEADS, HEAD_DIM).transpose(1, 0, 2)
    sink_heads = sink.reshape(KV_HEADS, group)
    attended = lax.map(lambda parts: attend_head(*parts), (query_heads, key_heads, value_heads, sink_heads))
    attended = attended.transpose(1, 0, 2).reshape(seq_len, HEADS * HEAD_DIM)
    chan_float = chan.astype(jnp.float32)
    running = jnp.concatenate([jnp.zeros((1, POOL_WIDTH), jnp.float32), jnp.cumsum(chan_float, axis=0)], axis=0)
    positions = jnp.arange(seq_len, dtype=jnp.int32)
    outputs = []
    for level in range(POOL_GROUPS):
        half = 2 ** level
        lower = jnp.clip(positions - half, 0, seq_len)
        upper = jnp.clip(positions + half, 0, seq_len)
        columns = slice(level * GROUP_DIM, (level + 1) * GROUP_DIM)
        band = running[:, columns]
        count = (upper - lower).astype(jnp.float32)
        spread = ((band[upper] - band[lower]) / count[:, None] - chan_float[:, columns]).astype(jnp.bfloat16)
        outputs.append(jnp.dot(spread, w_pool[level], preferred_element_type=jnp.float32))
    pooled = (jnp.concatenate(outputs, axis=1) * pool_scale).astype(jnp.bfloat16)
    attn_share = ATTN_WIDTH // N_TP
    pool_share = POOL_WIDTH // N_TP
    mix = jnp.zeros((seq_len, D), jnp.float32)
    for device in range(N_TP):
        attn_cols = slice(device * attn_share, (device + 1) * attn_share)
        pool_cols = slice(device * pool_share, (device + 1) * pool_share)
        partial_sum = jnp.dot(attended[:, attn_cols], w_out_attn[attn_cols], preferred_element_type=jnp.float32)
        partial_sum = partial_sum + jnp.dot(pooled[:, pool_cols], w_out_pool[pool_cols], preferred_element_type=jnp.float32)
        mix = mix + partial_sum.astype(jnp.bfloat16).astype(jnp.float32)
    row_mean = lax.optimization_barrier(jnp.sum(mix, axis=1)) / D
    variance = lax.optimization_barrier(jnp.sum(mix * mix, axis=1)) / D - row_mean * row_mean
    normed = (mix - row_mean[:, None]) * lax.rsqrt(variance + epsilon)[:, None] * out_gain
    return normed.astype(jnp.bfloat16)
```

```python
import jax
import jax.numpy as jnp
from jax import lax
from jax.sharding import PartitionSpec as P

HEAD_DIM = 64
POOL_GROUPS = 4
WINDOW = 128


epsilon = 1e-05
masked_score = -1e30
direct_limit = 8


def swap(value, axis, mask):
    count = lax.axis_size(axis)
    return lax.ppermute(value, axis, [(i, i ^ mask) for i in range(count)])


def spread_blocks(block):
    count = lax.axis_size("sp")
    near = {0: block}
    for mask in range(2, count, 2):
        near[mask] = swap(block, "sp", mask)
    parts = dict(near)
    for mask, part in near.items():
        parts[mask ^ 1] = swap(part, "sp", 1)
    return parts


def gather_rows(block):
    count = lax.axis_size("sp")
    if count > direct_limit or count & (count - 1):
        return lax.all_gather(block, "sp", axis=0, tiled=True)
    here = lax.axis_index("sp")
    rows = block.shape[0]
    whole = jnp.zeros((count * rows, block.shape[1]), block.dtype)
    for mask, part in spread_blocks(block).items():
        whole = lax.dynamic_update_slice_in_dim(whole, part, (here ^ mask) * rows, 0)
    return whole


def gather_tp(block):
    near = {0: block}
    step = 1
    count = lax.axis_size("tp")
    masks = []
    while step < count:
        masks.append(step)
        step *= 2
    for mask in reversed(masks):
        for known, part in list(near.items()):
            near[known ^ mask] = swap(part, "tp", mask)
    return near


def padded(cells, axis, width):
    count = lax.axis_size(axis)
    ends = count - 1
    head = lax.slice_in_dim(cells, 0, width, axis=0)
    tail = lax.slice_in_dim(cells, cells.shape[0] - width, cells.shape[0], axis=0)
    return jnp.concatenate(
        [
            lax.ppermute(tail, axis, [(i, i + 1) for i in range(ends)]),
            cells,
            lax.ppermute(head, axis, [(i + 1, i) for i in range(ends)]),
        ],
        axis=0,
    )


def attend_local(query, keys_ext, sinks, offset, seq_len, key_cols):
    tok_rows, query_cols = query.shape
    kv_local = key_cols // HEAD_DIM
    group = query_cols // key_cols
    block_count = tok_rows // WINDOW
    stacked = keys_ext.reshape(block_count + 2, WINDOW, 2 * key_cols)
    banded = jnp.concatenate([stacked[:-2], stacked[1:-1], stacked[2:]], axis=1)
    key_band = banded[:, :, :key_cols].reshape(block_count, 3 * WINDOW, kv_local, HEAD_DIM)
    value_band = banded[:, :, key_cols:].reshape(block_count, 3 * WINDOW, kv_local, HEAD_DIM)
    query_blocks = query.reshape(block_count, WINDOW, kv_local, group, HEAD_DIM)
    scores = jnp.einsum(
        "nqkgd,nskd->nkgqs", query_blocks, key_band, preferred_element_type=jnp.float32
    ) * HEAD_DIM ** (-0.5)
    starts = offset + jnp.arange(block_count, dtype=jnp.int32) * WINDOW
    query_pos = starts[:, None] + jnp.arange(WINDOW, dtype=jnp.int32)[None, :]
    key_pos = starts[:, None] + jnp.arange(3 * WINDOW, dtype=jnp.int32)[None, :] - WINDOW
    distance = key_pos[:, None, :] - query_pos[:, :, None]
    inside = (key_pos >= 0) & (key_pos < seq_len)
    keep = (jnp.abs(distance) <= WINDOW) & inside[:, None, :]
    scores = jnp.where(keep[:, None, None], scores, masked_score)
    sink_logit = sinks.reshape(kv_local, group)[None, :, :, None, None]
    top = jnp.maximum(jnp.max(scores, axis=-1, keepdims=True), sink_logit)
    raised = jnp.exp(scores - top)
    total = jnp.sum(raised, axis=-1, keepdims=True) + jnp.exp(sink_logit - top)
    probs = (raised / total).astype(jnp.bfloat16)
    attended = jnp.einsum(
        "nkgqs,nskd->nqkgd", probs, value_band, preferred_element_type=jnp.float32
    )
    return attended.astype(jnp.bfloat16).reshape(tok_rows, query_cols)


def pool_local(chan, w_pool, pool_scale, offset, seq_len):
    tok_rows, chan_cols = chan.shape
    rim_rows = 2 ** (POOL_GROUPS - 1)
    chan_ext = padded(chan, "sp", rim_rows)
    running = jnp.concatenate(
        [jnp.zeros((1, chan_cols), jnp.float32), jnp.cumsum(chan_ext.astype(jnp.float32), axis=0)],
        axis=0,
    )
    positions = offset + jnp.arange(tok_rows, dtype=jnp.int32)
    group_count = w_pool.shape[0]
    outputs = []
    wide = chan_cols // group_count
    for index in range(group_count):
        columns = slice(index * wide, (index + 1) * wide)
        half = jnp.left_shift(jnp.int32(1), lax.axis_index("tp") * group_count + index)
        upper = lax.dynamic_slice_in_dim(running, rim_rows + half, tok_rows, 0)[:, columns]
        lower = lax.dynamic_slice_in_dim(running, rim_rows - half, tok_rows, 0)[:, columns]
        count = (
            jnp.clip(positions + half, 0, seq_len) - jnp.clip(positions - half, 0, seq_len)
        ).astype(jnp.float32)
        spread = ((upper - lower) / count[:, None] - chan[:, columns].astype(jnp.float32)).astype(
            jnp.bfloat16
        )
        outputs.append(jnp.dot(spread, w_pool[index], preferred_element_type=jnp.float32))
    return (jnp.concatenate(outputs, axis=1) * pool_scale).astype(jnp.bfloat16)


def local(
    tokens,
    w_query,
    w_key,
    w_value,
    w_pool_in,
    sink,
    w_pool,
    pool_scale,
    w_out_attn,
    w_out_pool,
    out_gain,
):
    tok_rows, tok_cols = tokens.shape
    sp_count = lax.axis_size("sp")
    tp_count = lax.axis_size("tp")
    tp_here = lax.axis_index("tp")
    seq_len = tok_rows * sp_count
    offset = lax.axis_index("sp") * tok_rows
    key_cols = w_key.shape[1]
    query_cols = w_query.shape[1]

    joined = gather_rows(jnp.concatenate([w_key, w_value, w_query, w_pool_in], axis=1))

    whole = jnp.zeros((tok_rows, tok_cols * tp_count), tokens.dtype)
    for mask, part in gather_tp(tokens).items():
        whole = lax.dynamic_update_slice_in_dim(whole, part, (tp_here ^ mask) * tok_cols, 1)

    out_t = jnp.concatenate([w_out_attn, w_out_pool], axis=0).T
    out_cols, out_rows = out_t.shape
    slice_cols = out_cols // tp_count
    mine = jnp.zeros((slice_cols, out_rows * tp_count), out_t.dtype)
    for mask in range(tp_count):
        part = lax.dynamic_slice_in_dim(out_t, (tp_here ^ mask) * slice_cols, slice_cols, 0)
        if mask:
            part = swap(part, "tp", mask)
        mine = lax.dynamic_update_slice_in_dim(mine, part, (tp_here ^ mask) * out_rows, 1)
    out_whole = gather_rows(mine)

    sums = jnp.dot(whole, joined, preferred_element_type=jnp.float32).astype(jnp.bfloat16)
    key_value = sums[:, : 2 * key_cols]
    query = sums[:, 2 * key_cols : 2 * key_cols + query_cols]
    chan = sums[:, 2 * key_cols + query_cols :]
    keys_ext = padded(key_value, "sp", WINDOW)
    attended = attend_local(query, keys_ext, sink, offset, seq_len, key_cols)
    pooled = pool_local(chan, w_pool, pool_scale, offset, seq_len)

    attended_parts = gather_tp(attended)
    pooled_parts = gather_tp(pooled)
    mix = None
    for mask in attended_parts:
        hidden = jnp.concatenate([attended_parts[mask], pooled_parts[mask]], axis=1)
        rows = lax.dynamic_slice_in_dim(out_whole, (tp_here ^ mask) * out_rows, out_rows, 1)
        partial = lax.dot_general(
            hidden, rows, (((1,), (1,)), ((), ())), preferred_element_type=jnp.float32
        ).astype(jnp.bfloat16)
        mix = partial.astype(jnp.float32) if mix is None else mix + partial.astype(jnp.float32)

    stats = jnp.stack([jnp.sum(mix, axis=1), jnp.sum(mix * mix, axis=1)])
    row_total, row_square = stats + sum(swap(stats, "tp", mask) for mask in range(1, tp_count))
    model_width = out_gain.shape[0] * tp_count
    row_mean = row_total / model_width
    variance = row_square / model_width - row_mean * row_mean

    share_cols = mix.shape[1] // tp_count
    rounded = mix.astype(jnp.bfloat16)
    pieces = jnp.zeros((tp_count, tok_rows, share_cols), jnp.bfloat16)
    for mask in range(tp_count):
        part = lax.dynamic_slice_in_dim(rounded, (tp_here ^ mask) * share_cols, share_cols, 1)
        if mask:
            part = swap(part, "tp", mask)
        pieces = lax.dynamic_update_slice_in_dim(pieces, part[None], tp_here ^ mask, 0)
    share = pieces.reshape(tp_count, tok_rows, share_cols // slice_cols, slice_cols)
    share = share.transpose(1, 2, 0, 3).reshape(tok_rows, share_cols * tp_count).astype(jnp.float32)
    normed = (share - row_mean[:, None]) * lax.rsqrt(variance + epsilon)[:, None] * out_gain
    return normed.astype(jnp.bfloat16)


def solution(mesh):
    return jax.shard_map(
        local,
        mesh=mesh,
        in_specs=(
            P("sp", "tp"),
            P("sp", "tp"),
            P("sp", "tp"),
            P("sp", "tp"),
            P("sp", "tp"),
            P("tp"),
            P("tp", None, None),
            P("tp"),
            P("tp", "sp"),
            P("tp", "sp"),
            P("tp"),
        ),
        out_specs=P("sp", "tp"),
        check_vma=False,
    )
```

```python
import jax
import jax.numpy as jnp
from jax import lax
from jax.experimental import pallas as pl
from jax.experimental.pallas import tpu as pltpu
from jax.sharding import PartitionSpec as P


HEAD_DIM = 64
POOL_GROUPS = 4
WINDOW = 128
TILE = 128


epsilon = 1e-05
masked_score = -1e30
direct_limit = 8

VMEM = pl.BlockSpec(memory_space=pltpu.VMEM)
SMEM = pl.BlockSpec(memory_space=pltpu.SMEM)


def call(body, operands, outs, scratch=(), flops=0, specs=None):
    moved = sum(x.size * x.dtype.itemsize for x in operands)
    many = isinstance(outs, list)
    return pl.pallas_call(
        body,
        out_shape=outs,
        in_specs=specs or [VMEM] * len(operands),
        out_specs=[VMEM] * len(outs) if many else VMEM,
        scratch_shapes=list(scratch),
        cost_estimate=pl.CostEstimate(flops=flops, bytes_accessed=moved, transcendentals=0),
    )(*operands)


def shape(dims, dtype=jnp.bfloat16):
    return jax.ShapeDtypeStruct(dims, dtype)


def at(index, size):
    return pl.ds(pl.multiple_of(index * size, size), size)


def swap(value, axis, mask):
    count = lax.axis_size(axis)
    return lax.ppermute(value, axis, [(i, i ^ mask) for i in range(count)])


def gather_sp(block):
    count = lax.axis_size("sp")
    if count > direct_limit or count & (count - 1):
        return {None: lax.all_gather(block, "sp", axis=0, tiled=True)}
    near = {0: block}
    for mask in range(2, count, 2):
        near[mask] = swap(block, "sp", mask)
    parts = dict(near)
    for mask, part in near.items():
        parts[mask ^ 1] = swap(part, "sp", 1)
    return parts


def gather_tp(block):
    count = lax.axis_size("tp")
    near = {0: block}
    mask = count // 2
    while mask:
        for known, part in list(near.items()):
            near[known ^ mask] = swap(part, "tp", mask)
        mask //= 2
    return near


def rims(cells, width):
    ends = lax.axis_size("sp") - 1
    rows = cells.shape[0]
    above = lax.ppermute(cells[rows - width :], "sp", [(i, i + 1) for i in range(ends)])
    below = lax.ppermute(cells[:width], "sp", [(i + 1, i) for i in range(ends)])
    return above, below


def place(parts, refs, store):
    here = lax.axis_index("sp")
    for mask, ref in zip(parts, refs):
        rows = ref.shape[0]
        if mask is None:
            store[...] = ref[...]
        else:
            store[at(here ^ mask, rows), :] = ref[...]


def prepare(w_query, w_key, w_value, w_pool_in, w_out_attn, w_out_pool):
    rows = w_query.shape[0]
    out_cols = w_out_attn.shape[1]
    if rows % 16 or out_cols % 128:
        joined = jnp.concatenate([w_key, w_value, w_query, w_pool_in], axis=1)
        return joined, jnp.concatenate([w_out_attn, w_out_pool], axis=0).T

    def body(q_ref, k_ref, v_ref, p_ref, a_ref, b_ref, joined_ref, out_ref):
        joined_ref[...] = jnp.concatenate([k_ref[...], v_ref[...], q_ref[...], p_ref[...]], axis=1)
        out_ref[...] = jnp.concatenate([a_ref[...].T, b_ref[...].T], axis=1)

    operands = (w_query, w_key, w_value, w_pool_in, w_out_attn, w_out_pool)
    wide = sum(x.shape[1] for x in operands[:4])
    tall = w_out_attn.shape[0] + w_out_pool.shape[0]
    return call(body, operands, [shape((rows, wide)), shape((out_cols, tall))])


def project(tokens, weights, widths):
    parts = list(weights)
    masks = list(tokens)
    tok_rows, tok_cols = tokens[0].shape
    wide = sum(widths)
    total = tok_cols * len(masks)
    tile = min(TILE, tok_rows)

    def body(*refs):
        tok_refs = refs[: len(masks)]
        w_refs = refs[len(masks) : len(masks) + len(parts)]
        outs = refs[len(masks) + len(parts) : -1]
        store = refs[-1]
        here = lax.axis_index("tp")
        place(parts, w_refs, store)

        def step(i, carry):
            rows = at(i, tile)
            acc = None
            for mask, ref in zip(masks, tok_refs):
                part = jnp.dot(
                    ref[rows, :],
                    store[at(here ^ mask, tok_cols), :],
                    preferred_element_type=jnp.float32,
                )
                acc = part if acc is None else acc + part
            acc = acc.astype(jnp.bfloat16)
            start = 0
            for out, width in zip(outs, widths):
                out[rows, :] = acc[:, start : start + width]
                start += width
            return carry

        lax.fori_loop(0, tok_rows // tile, step, 0)

    operands = [tokens[m] for m in masks] + [weights[m] for m in parts]
    return call(
        body,
        operands,
        [shape((tok_rows, width)) for width in widths],
        [pltpu.VMEM((total, wide), jnp.bfloat16)],
        2 * tok_rows * total * wide,
    )


def attend(query, key_value, above, below, sinks, key_cols, seq_len):
    tok_rows, query_cols = query.shape
    kv_local = key_cols // HEAD_DIM
    group = query_cols // key_cols
    blocks = tok_rows // WINDOW
    span = 3 * WINDOW

    def body(q_ref, kv_ref, up_ref, down_ref, sink_ref, out_ref, store):
        offset = lax.axis_index("sp") * tok_rows
        store[0:WINDOW, :] = up_ref[...]
        store[WINDOW : WINDOW + tok_rows, :] = kv_ref[...]
        store[WINDOW + tok_rows :, :] = down_ref[...]
        row = lax.broadcasted_iota(jnp.int32, (WINDOW, span), 0)
        col = lax.broadcasted_iota(jnp.int32, (WINDOW, span), 1)
        near = jnp.abs(col - WINDOW - row) <= WINDOW

        def step(b, carry):
            start = pl.multiple_of(b * WINDOW, WINDOW)
            key_pos = col + (offset + start - WINDOW)
            keep = near & (key_pos >= 0) & (key_pos < seq_len)
            band = store[pl.ds(start, span), :]
            query_rows = q_ref[pl.ds(start, WINDOW), :]
            pieces = []
            for kv in range(kv_local):
                keys = band[:, kv * HEAD_DIM : (kv + 1) * HEAD_DIM]
                values = band[:, key_cols + kv * HEAD_DIM : key_cols + (kv + 1) * HEAD_DIM]
                for member in range(group):
                    head = kv * group + member
                    scores = lax.dot_general(
                        query_rows[:, head * HEAD_DIM : (head + 1) * HEAD_DIM],
                        keys,
                        (((1,), (1,)), ((), ())),
                        preferred_element_type=jnp.float32,
                    ) * HEAD_DIM ** (-0.5)
                    scores = jnp.where(keep, scores, masked_score)
                    sink = sink_ref[head]
                    top = jnp.maximum(jnp.max(scores, axis=1, keepdims=True), sink)
                    raised = jnp.exp(scores - top)
                    whole = jnp.sum(raised, axis=1, keepdims=True) + jnp.exp(sink - top)
                    probs = (raised * (1.0 / whole)).astype(jnp.bfloat16)
                    pieces.append(
                        jnp.dot(probs, values, preferred_element_type=jnp.float32).astype(
                            jnp.bfloat16
                        )
                    )
            out_ref[pl.ds(start, WINDOW), :] = jnp.concatenate(pieces, axis=1)
            return carry

        lax.fori_loop(0, blocks, step, 0)

    return call(
        body,
        [query, key_value, above, below, sinks],
        shape((tok_rows, query_cols)),
        [pltpu.VMEM((tok_rows + 2 * WINDOW, 2 * key_cols), jnp.bfloat16)],
        4 * tok_rows * span * query_cols,
        [VMEM] * 4 + [SMEM],
    )


def pool(chan, above, below, w_pool, pool_scale, seq_len):
    tok_rows, chan_cols = chan.shape
    rim = above.shape[0]
    groups = w_pool.shape[0]
    wide = chan_cols // groups
    full = tok_rows + 2 * rim

    def body(chan_ref, up_ref, down_ref, w_ref, scale_ref, out_ref):
        first = lax.axis_index("tp") * groups
        offset = lax.axis_index("sp") * tok_rows
        for g in range(groups):
            cols = slice(g * wide, (g + 1) * wide)
            own = chan_ref[:, cols].astype(jnp.float32)
            cells = jnp.concatenate(
                [
                    up_ref[:, cols].astype(jnp.float32),
                    own,
                    down_ref[:, cols].astype(jnp.float32),
                ],
                axis=0,
            )
            level = first + g
            run = cells + pltpu.roll(cells, 1, 0)
            window = run
            for step in range(1, POOL_GROUPS):
                reach = 2 ** (step - 1)
                run = pltpu.roll(run, reach, 0) + pltpu.roll(run, full - reach, 0)
                window = jnp.where(level >= step, run, window)
            window = window[rim : rim + tok_rows]
            half = jnp.left_shift(jnp.int32(1), level)
            position = lax.broadcasted_iota(jnp.int32, (tok_rows, 1), 0) + offset
            count = jnp.minimum(position + half, seq_len) - jnp.maximum(position - half, 0)
            spread = (window / count.astype(jnp.float32) - own).astype(jnp.bfloat16)
            mapped = jnp.dot(spread, w_ref[g], preferred_element_type=jnp.float32)
            out_ref[:, cols] = (mapped * scale_ref[:, cols]).astype(jnp.bfloat16)

    return call(
        body,
        [chan, above, below, w_pool, pool_scale.reshape(1, chan_cols)],
        shape((tok_rows, chan_cols)),
        (),
        2 * tok_rows * wide * chan_cols,
    )


def mix_out(attended, pooled, weights):
    masks = list(attended)
    parts = list(weights)
    tok_rows, attn_cols = attended[0].shape
    pool_cols = pooled[0].shape[1]
    depth = attn_cols + pool_cols
    total = depth * len(masks)
    cols = sum(weights[m].shape[0] for m in parts)
    share = cols // len(masks)
    tile = min(TILE, tok_rows)
    contract = (((1,), (1,)), ((), ()))

    def body(*refs):
        n = len(masks)
        attn_refs, pool_refs = refs[:n], refs[n : 2 * n]
        w_refs = refs[2 * n : 2 * n + len(parts)]
        piece_refs = refs[2 * n + len(parts) : 3 * n + len(parts)]
        stats_ref, store = refs[-2:]
        here = lax.axis_index("tp")
        place(parts, w_refs, store)

        def step(i, carry):
            rows = at(i, tile)
            mix = None
            for mask, a_ref, p_ref in zip(masks, attn_refs, pool_refs):
                base = pl.multiple_of((here ^ mask) * depth, depth)
                partial = lax.dot_general(
                    a_ref[rows, :],
                    store[:, pl.ds(base, attn_cols)],
                    contract,
                    preferred_element_type=jnp.float32,
                ) + lax.dot_general(
                    p_ref[rows, :],
                    store[:, pl.ds(pl.multiple_of(base + attn_cols, 128), pool_cols)],
                    contract,
                    preferred_element_type=jnp.float32,
                )
                partial = partial.astype(jnp.bfloat16).astype(jnp.float32)
                mix = partial if mix is None else mix + partial

            def folded(values):
                lanes = sum(values[:, k * 128 : (k + 1) * 128] for k in range(cols // 128))
                return jnp.sum(lanes.T, axis=0, keepdims=True)

            stats_ref[0:1, rows] = folded(mix)
            stats_ref[1:2, rows] = folded(mix * mix)
            whole = mix.astype(jnp.bfloat16)
            for k in range(n):
                piece_refs_k = whole[:, k * share : (k + 1) * share]
                for mask, ref in zip(masks, piece_refs):
                    @pl.when((here ^ mask) == k)
                    def _():
                        ref[rows, :] = piece_refs_k

            return carry

        lax.fori_loop(0, tok_rows // tile, step, 0)

    operands = (
        [attended[m] for m in masks] + [pooled[m] for m in masks] + [weights[m] for m in parts]
    )
    results = call(
        body,
        operands,
        [shape((tok_rows, share)) for _ in masks] + [shape((2, tok_rows), jnp.float32)],
        [pltpu.VMEM((cols, total), jnp.bfloat16)],
        2 * tok_rows * total * cols,
    )
    return dict(zip(masks, results[:-1])), results[-1]


def close(pieces, stats, out_gain, slice_cols):
    masks = list(pieces)
    tok_rows, share = pieces[0].shape
    width = out_gain.shape[0]
    model_width = width * len(masks)
    if slice_cols % 64:
        here = lax.axis_index("tp")
        stacked = jnp.zeros((len(masks), tok_rows, share), jnp.bfloat16)
        for mask, part in pieces.items():
            stacked = lax.dynamic_update_slice_in_dim(stacked, part[None], here ^ mask, 0)
        grid = stacked.reshape(len(masks), tok_rows, share // slice_cols, slice_cols)
        mixed = grid.transpose(1, 2, 0, 3).reshape(tok_rows, width).astype(jnp.float32)
        row_total, row_square = sum(stats.values())
        row_mean = row_total / model_width
        variance = row_square / model_width - row_mean * row_mean
        normed = (mixed - row_mean[:, None]) * lax.rsqrt(variance + epsilon)[:, None] * out_gain
        return normed.astype(jnp.bfloat16)

    tile = min(TILE, tok_rows)

    def body(*refs):
        n = len(masks)
        piece_refs, stat_refs = refs[:n], refs[n : 2 * n]
        gain_ref, out_ref, store = refs[2 * n :]
        here = lax.axis_index("tp")
        for mask, ref in zip(masks, piece_refs):
            store[here ^ mask] = ref[...]

        def step(i, carry):
            rows = at(i, tile)
            sums = stat_refs[0][:, rows]
            for ref in stat_refs[1:]:
                sums = sums + ref[:, rows]
            mean = sums[0:1] / model_width
            scale = lax.rsqrt(sums[1:2] / model_width - mean * mean + epsilon)
            mean = jnp.broadcast_to(mean, (128, tile)).T[:, 0:1]
            scale = jnp.broadcast_to(scale, (128, tile)).T[:, 0:1]
            parts = []
            for block in range(share // slice_cols):
                cols = slice(block * slice_cols, (block + 1) * slice_cols)
                parts += [store[k, rows, :][:, cols] for k in range(n)]
            mixed = jnp.concatenate(parts, axis=1).astype(jnp.float32)
            out_ref[rows, :] = ((mixed - mean) * scale * gain_ref[...]).astype(jnp.bfloat16)
            return carry

        lax.fori_loop(0, tok_rows // tile, step, 0)

    return call(
        body,
        [pieces[m] for m in masks] + [stats[m] for m in masks] + [out_gain.reshape(1, width)],
        shape((tok_rows, width)),
        [pltpu.VMEM((len(masks), tok_rows, share), jnp.bfloat16)],
        8 * tok_rows * width,
    )


def local(
    tokens,
    w_query,
    w_key,
    w_value,
    w_pool_in,
    sink,
    w_pool,
    pool_scale,
    w_out_attn,
    w_out_pool,
    out_gain,
):
    tok_rows = tokens.shape[0]
    tp_count = lax.axis_size("tp")
    tp_here = lax.axis_index("tp")
    seq_len = tok_rows * lax.axis_size("sp")
    key_cols = w_key.shape[1]

    all_tokens = gather_tp(tokens)
    joined, out_t = prepare(w_query, w_key, w_value, w_pool_in, w_out_attn, w_out_pool)
    weights = gather_sp(joined)

    out_cols, out_rows = out_t.shape
    slice_cols = out_cols // tp_count
    mine = jnp.zeros((slice_cols, out_rows * tp_count), out_t.dtype)
    for mask in range(tp_count):
        part = lax.dynamic_slice_in_dim(out_t, (tp_here ^ mask) * slice_cols, slice_cols, 0)
        if mask:
            part = swap(part, "tp", mask)
        mine = lax.dynamic_update_slice_in_dim(mine, part, (tp_here ^ mask) * out_rows, 1)
    out_weights = gather_sp(mine)

    key_value, query, chan = project(
        all_tokens, weights, [2 * key_cols, w_query.shape[1], w_pool_in.shape[1]]
    )
    attended = attend(query, key_value, *rims(key_value, WINDOW), sink, key_cols, seq_len)
    pooled = pool(chan, *rims(chan, 2 ** (POOL_GROUPS - 1)), w_pool, pool_scale, seq_len)
    pieces, stats = mix_out(gather_tp(attended), gather_tp(pooled), out_weights)
    stats = {m: stats if m == 0 else swap(stats, "tp", m) for m in pieces}
    pieces = {m: p if m == 0 else swap(p, "tp", m) for m, p in pieces.items()}
    return close(pieces, stats, out_gain, slice_cols)


def solution(mesh):
    return jax.shard_map(
        local,
        mesh=mesh,
        in_specs=(
            P("sp", "tp"),
            P("sp", "tp"),
            P("sp", "tp"),
            P("sp", "tp"),
            P("sp", "tp"),
            P("tp"),
            P("tp", None, None),
            P("tp"),
            P("tp", "sp"),
            P("tp", "sp"),
            P("tp"),
        ),
        out_specs=P("sp", "tp"),
        check_vma=False,
    )
```

```python
import jax
import jax.numpy as jnp
from jax import lax
from jax.experimental import pallas as pl
from jax.experimental.pallas import tpu as pltpu
from jax.sharding import PartitionSpec as P


HEAD_DIM = 64
POOL_GROUPS = 4
WINDOW = 128
TILE = 128


epsilon = 1e-05
masked_score = -1e30
direct_limit = 8
kernel_bytes = 16 * 2**20

VMEM = pl.BlockSpec(memory_space=pltpu.VMEM)
SMEM = pl.BlockSpec(memory_space=pltpu.SMEM)


def call(body, operands, outs, scratch=(), flops=0, specs=None):
    moved = sum(x.size * x.dtype.itemsize for x in operands)
    many = isinstance(outs, list)
    return pl.pallas_call(
        body,
        out_shape=outs,
        in_specs=specs or [VMEM] * len(operands),
        out_specs=[VMEM] * len(outs) if many else VMEM,
        scratch_shapes=list(scratch),
        cost_estimate=pl.CostEstimate(flops=flops, bytes_accessed=moved, transcendentals=0),
        compiler_params=pltpu.CompilerParams(vmem_limit_bytes=kernel_bytes),
    )(*operands)


def shape(dims, dtype=jnp.bfloat16):
    return jax.ShapeDtypeStruct(dims, dtype)


def at(index, size):
    return pl.ds(pl.multiple_of(index * size, size), size)


def swap(value, axis, mask):
    count = lax.axis_size(axis)
    return lax.ppermute(value, axis, [(i, i ^ mask) for i in range(count)])


def gather_sp(block):
    count = lax.axis_size("sp")
    if count > direct_limit or count & (count - 1):
        return {None: lax.all_gather(block, "sp", axis=0, tiled=True)}
    near = {0: block}
    for mask in range(2, count, 2):
        near[mask] = swap(block, "sp", mask)
    parts = dict(near)
    for mask, part in near.items():
        parts[mask ^ 1] = swap(part, "sp", 1)
    return parts


def gather_tp(block):
    count = lax.axis_size("tp")
    near = {0: block}
    mask = count // 2
    while mask:
        for known, part in list(near.items()):
            near[known ^ mask] = swap(part, "tp", mask)
        mask //= 2
    return near


def exchange(head, tail):
    ends = lax.axis_size("sp") - 1
    above = lax.ppermute(tail, "sp", [(i, i + 1) for i in range(ends)])
    below = lax.ppermute(head, "sp", [(i + 1, i) for i in range(ends)])
    return above, below


def place(parts, refs, store):
    here = lax.axis_index("sp")
    for mask, ref in zip(parts, refs):
        rows = ref.shape[0]
        if mask is None:
            store[...] = ref[...]
        else:
            store[at(here ^ mask, rows), :] = ref[...]


def pack_in(w_query, w_key, w_value, w_pool_in):
    rows = w_query.shape[0]
    if rows % 128:
        return jnp.concatenate([w_key, w_value, w_query, w_pool_in], axis=1)

    def body(q_ref, k_ref, v_ref, p_ref, joined_ref):
        joined_ref[...] = jnp.concatenate(
            [k_ref[...].T, v_ref[...].T, q_ref[...], p_ref[...]], axis=1
        )

    wide = w_query.shape[1] + w_key.shape[1] + w_value.shape[1] + w_pool_in.shape[1]
    operands = [w_query, w_key.T, w_value.T, w_pool_in]
    return call(body, operands, shape((rows, wide)))


def pack_out(w_out_attn, w_out_pool, tp_count):
    out_cols = w_out_attn.shape[1]
    depth = w_out_attn.shape[0] + w_out_pool.shape[0]
    width = out_cols // tp_count
    if out_cols % 128 or width % 16:
        whole = jnp.concatenate([w_out_attn, w_out_pool], axis=0).T
        here = lax.axis_index("tp")
        return [
            lax.dynamic_slice_in_dim(whole, (here ^ mask) * width, width, 0)
            for mask in range(tp_count)
        ]

    def body(a_ref, b_ref, *refs):
        store = refs[-1]
        here = lax.axis_index("tp")
        store[...] = jnp.concatenate([a_ref[...].T, b_ref[...].T], axis=1)
        for mask, ref in enumerate(refs[:-1]):
            ref[...] = store[at(here ^ mask, width), :]

    return call(
        body,
        [w_out_attn, w_out_pool],
        [shape((width, depth)) for _ in range(tp_count)],
        [pltpu.VMEM((out_cols, depth), jnp.bfloat16)],
    )


def project(tokens, weights, widths, rim):
    parts = list(weights)
    masks = list(tokens)
    tok_rows, tok_cols = tokens[0].shape
    wide = sum(widths)
    total = tok_cols * len(masks)
    tile = min(TILE, tok_rows)
    lanes = widths[0]
    pack_rows = WINDOW + rim * (widths[2] // lanes)

    def body(*refs):
        tok_refs = refs[: len(masks)]
        w_refs = refs[len(masks) : len(masks) + len(parts)]
        outs = refs[len(masks) + len(parts) : -3]
        head_ref, tail_ref, store = refs[-3:]
        here = lax.axis_index("tp")
        place(parts, w_refs, store)

        def step(i, carry):
            rows = at(i, tile)
            acc = None
            for mask, ref in zip(masks, tok_refs):
                part = jnp.dot(
                    ref[rows, :],
                    store[at(here ^ mask, tok_cols), :],
                    preferred_element_type=jnp.float32,
                )
                acc = part if acc is None else acc + part
            acc = acc.astype(jnp.bfloat16)
            start = 0
            for out, width in zip(outs, widths):
                out[rows, :] = acc[:, start : start + width]
                start += width
            return carry

        lax.fori_loop(0, tok_rows // tile, step, 0)
        for ref, kv_start, rim_start in (
            (head_ref, 0, 0),
            (tail_ref, tok_rows - WINDOW, tok_rows - rim),
        ):
            ref[0:WINDOW, :] = outs[0][kv_start : kv_start + WINDOW, :]
            edge = outs[2][rim_start : rim_start + rim, :].astype(jnp.float32)
            ref[WINDOW:pack_rows, :] = jnp.concatenate(
                [edge[:, c : c + lanes] for c in range(0, widths[2], lanes)], axis=0
            ).astype(jnp.bfloat16)

    operands = [tokens[m] for m in masks] + [weights[m] for m in parts]
    return call(
        body,
        operands,
        [shape((tok_rows, width)) for width in widths] + [shape((pack_rows, lanes))] * 2,
        [pltpu.VMEM((total, wide), jnp.bfloat16)],
        2 * tok_rows * total * wide,
    )


def attend(query, key_value, above, below, sinks, key_cols, seq_len):
    tok_rows, query_cols = query.shape
    kv_local = key_cols // HEAD_DIM
    group = query_cols // key_cols
    blocks = tok_rows // WINDOW
    span = 3 * WINDOW
    root = HEAD_DIM**0.5
    rate = 1.4426950408889634 / root

    def body(q_ref, kv_ref, up_ref, down_ref, sink_ref, out_ref, store, turned):
        offset = lax.axis_index("sp") * tok_rows
        store[0:WINDOW, :] = up_ref[0:WINDOW, :]
        store[WINDOW : WINDOW + tok_rows, :] = kv_ref[...]
        store[WINDOW + tok_rows :, :] = down_ref[0:WINDOW, :]
        for b in range(blocks + 2):
            rows = slice(b * WINDOW, (b + 1) * WINDOW)
            turned[:, rows] = store[rows, :].T
        key_row = lax.broadcasted_iota(jnp.int32, (WINDOW, WINDOW), 0)
        query_col = lax.broadcasted_iota(jnp.int32, (WINDOW, WINDOW), 1)

        for b in range(blocks):
            rows = slice(b * WINDOW, (b + 1) * WINDOW)
            keep_first = key_row >= query_col
            keep_last = key_row <= query_col
            if b == 0:
                keep_first &= offset > 0
            if b == blocks - 1:
                keep_last &= offset + tok_rows < seq_len
            query_turned = q_ref[rows, :].T
            pieces = []
            for kv in range(kv_local):
                lane = slice(kv * HEAD_DIM, (kv + 1) * HEAD_DIM)
                keys = store[b * WINDOW : b * WINDOW + span, lane]
                values = turned[
                    key_cols + kv * HEAD_DIM : key_cols + (kv + 1) * HEAD_DIM,
                    b * WINDOW : b * WINDOW + span,
                ]
                for member in range(group):
                    head = kv * group + member
                    scores = jnp.dot(
                        keys,
                        query_turned[head * HEAD_DIM : (head + 1) * HEAD_DIM, :],
                        preferred_element_type=jnp.float32,
                    )
                    scores = jnp.concatenate(
                        [
                            jnp.where(keep_first, scores[:WINDOW], masked_score),
                            scores[WINDOW : 2 * WINDOW],
                            jnp.where(keep_last, scores[2 * WINDOW :], masked_score),
                        ],
                        axis=0,
                    )
                    sink = sink_ref[head] * root
                    top = jnp.maximum(jnp.max(scores, axis=0, keepdims=True), sink)
                    raised = jnp.exp2((scores - top) * rate)
                    whole = jnp.sum(raised, axis=0, keepdims=True) + jnp.exp2((sink - top) * rate)
                    probs = (raised * (1.0 / whole)).astype(jnp.bfloat16)
                    pieces.append(jnp.dot(values, probs, preferred_element_type=jnp.float32))
            out_ref[rows, :] = jnp.concatenate(pieces, axis=0).T.astype(jnp.bfloat16)

    return call(
        body,
        [query, key_value, above, below, sinks],
        shape((tok_rows, query_cols)),
        [
            pltpu.VMEM((tok_rows + 2 * WINDOW, 2 * key_cols), jnp.bfloat16),
            pltpu.VMEM((2 * key_cols, tok_rows + 2 * WINDOW), jnp.bfloat16),
        ],
        4 * tok_rows * span * query_cols,
        [VMEM] * 4 + [SMEM],
    )


def pool(chan, above, below, w_pool, pool_scale, seq_len):
    tok_rows, chan_cols = chan.shape
    lanes = above.shape[1]
    rim = (above.shape[0] - WINDOW) * lanes // chan_cols
    groups = w_pool.shape[0]
    wide = chan_cols // groups
    full = tok_rows + 2 * rim

    def edge(ref):
        rows = ref[WINDOW:, :].astype(jnp.float32)
        return jnp.concatenate(
            [rows[c * rim : (c + 1) * rim] for c in range(chan_cols // lanes)], axis=1
        )

    def body(chan_ref, up_ref, down_ref, w_ref, scale_ref, out_ref):
        up, down = edge(up_ref), edge(down_ref)
        first = lax.axis_index("tp") * groups
        offset = lax.axis_index("sp") * tok_rows
        for g in range(groups):
            cols = slice(g * wide, (g + 1) * wide)
            own = chan_ref[:, cols].astype(jnp.float32)
            cells = jnp.concatenate([up[:, cols], own, down[:, cols]], axis=0)
            level = first + g
            run = cells + pltpu.roll(cells, 1, 0)
            window = run
            for step in range(1, POOL_GROUPS):
                reach = 2 ** (step - 1)
                run = pltpu.roll(run, reach, 0) + pltpu.roll(run, full - reach, 0)
                window = jnp.where(level >= step, run, window)
            window = window[rim : rim + tok_rows]
            half = jnp.left_shift(jnp.int32(1), level)
            position = lax.broadcasted_iota(jnp.int32, (tok_rows, 1), 0) + offset
            count = jnp.minimum(position + half, seq_len) - jnp.maximum(position - half, 0)
            spread = (window / count.astype(jnp.float32) - own).astype(jnp.bfloat16)
            mapped = jnp.dot(spread, w_ref[g], preferred_element_type=jnp.float32)
            out_ref[:, cols] = (mapped * scale_ref[:, cols]).astype(jnp.bfloat16)

    return call(
        body,
        [chan, above, below, w_pool, pool_scale.reshape(1, chan_cols)],
        shape((tok_rows, chan_cols)),
        (),
        2 * tok_rows * wide * chan_cols,
    )


def mix_out(attended, pooled, weights):
    masks = list(attended)
    parts = list(weights)
    tok_rows, attn_cols = attended[0].shape
    pool_cols = pooled[0].shape[1]
    depth = attn_cols + pool_cols
    total = depth * len(masks)
    cols = sum(weights[m].shape[0] for m in parts)
    share = cols // len(masks)
    tile = min(TILE, tok_rows)
    contract = (((1,), (1,)), ((), ()))

    def body(*refs):
        n = len(masks)
        attn_refs, pool_refs = refs[:n], refs[n : 2 * n]
        w_refs = refs[2 * n : 2 * n + len(parts)]
        piece_refs = refs[2 * n + len(parts) : 3 * n + len(parts)]
        sums, store = refs[-2:]
        here = lax.axis_index("tp")
        place(parts, w_refs, store)

        def step(i, carry):
            rows = at(i, tile)
            mix = None
            for mask, a_ref, p_ref in zip(masks, attn_refs, pool_refs):
                base = pl.multiple_of((here ^ mask) * depth, depth)
                partial = lax.dot_general(
                    a_ref[rows, :],
                    store[:, pl.ds(base, attn_cols)],
                    contract,
                    preferred_element_type=jnp.float32,
                ) + lax.dot_general(
                    p_ref[rows, :],
                    store[:, pl.ds(pl.multiple_of(base + attn_cols, 128), pool_cols)],
                    contract,
                    preferred_element_type=jnp.float32,
                )
                partial = partial.astype(jnp.bfloat16).astype(jnp.float32)
                mix = partial if mix is None else mix + partial

            def folded(values):
                lanes = sum(values[:, k * 128 : (k + 1) * 128] for k in range(cols // 128))
                return jnp.sum(lanes.T, axis=0, keepdims=True)

            terms = []
            for rest in (folded(mix), folded(mix * mix)):
                for _ in range(3):
                    term = rest.astype(jnp.bfloat16).astype(jnp.float32)
                    terms.append(term)
                    rest = rest - term
            terms.append(jnp.zeros((2, tile), jnp.float32))
            sums[at(i, 8), :] = jnp.concatenate(terms, axis=0)
            whole = mix.astype(jnp.bfloat16)
            for k in range(n):
                piece_refs_k = whole[:, k * share : (k + 1) * share]
                for mask, ref in zip(masks, piece_refs):
                    @pl.when((here ^ mask) == k)
                    def _():
                        ref[rows, :] = piece_refs_k

            return carry

        lax.fori_loop(0, tok_rows // tile, step, 0)
        for ref in piece_refs:
            ref[tok_rows:, :] = sums[...].astype(jnp.bfloat16)

    operands = (
        [attended[m] for m in masks] + [pooled[m] for m in masks] + [weights[m] for m in parts]
    )
    extra = 8 * (tok_rows // tile)
    results = call(
        body,
        operands,
        [shape((tok_rows + extra, share)) for _ in masks],
        [pltpu.VMEM((extra, tile), jnp.float32), pltpu.VMEM((cols, total), jnp.bfloat16)],
        2 * tok_rows * total * cols,
    )
    return dict(zip(masks, results))


def close(pieces, out_gain, tok_rows, slice_cols):
    masks = list(pieces)
    held, share = pieces[0].shape
    width = out_gain.shape[0]
    model_width = width * len(masks)
    tile = min(TILE, tok_rows)

    def moments(sums):
        mean = sum(sums[k : k + 1] for k in range(3)) / model_width
        square = sum(sums[k : k + 1] for k in range(3, 6)) / model_width
        return mean, lax.rsqrt(square - mean * mean + epsilon)

    if slice_cols % 64:
        here = lax.axis_index("tp")
        stacked = jnp.zeros((len(masks), held, share), jnp.bfloat16)
        for mask, part in pieces.items():
            stacked = lax.dynamic_update_slice_in_dim(stacked, part[None], here ^ mask, 0)
        sums = jnp.sum(stacked[:, tok_rows:].astype(jnp.float32), axis=0)
        mean, scale = moments(sums.reshape(-1, 8, tile).transpose(1, 0, 2).reshape(8, -1))
        grid = stacked[:, :tok_rows].reshape(len(masks), tok_rows, -1, slice_cols)
        mixed = grid.transpose(1, 2, 0, 3).reshape(tok_rows, width).astype(jnp.float32)
        return ((mixed - mean.T) * scale.T * out_gain).astype(jnp.bfloat16)

    def body(*refs):
        n = len(masks)
        piece_refs = refs[:n]
        gain_ref, out_ref, store = refs[n:]
        here = lax.axis_index("tp")
        total = None
        for mask, ref in zip(masks, piece_refs):
            store[here ^ mask] = ref[0:tok_rows, :]
            sums = ref[tok_rows:, :].astype(jnp.float32)
            total = sums if total is None else total + sums
        for i in range(tok_rows // tile):
            rows = slice(i * tile, (i + 1) * tile)
            mean, scale = moments(total[8 * i : 8 * (i + 1)])
            mean = jnp.broadcast_to(mean, (128, tile)).T[:, 0:1]
            scale = jnp.broadcast_to(scale, (128, tile)).T[:, 0:1]
            parts = []
            for block in range(share // slice_cols):
                cols = slice(block * slice_cols, (block + 1) * slice_cols)
                parts += [store[k, rows, cols] for k in range(n)]
            mixed = jnp.concatenate(parts, axis=1).astype(jnp.float32)
            out_ref[rows, :] = ((mixed - mean) * scale * gain_ref[...]).astype(jnp.bfloat16)

    return call(
        body,
        [pieces[m] for m in masks] + [out_gain.reshape(1, width)],
        shape((tok_rows, width)),
        [pltpu.VMEM((len(masks), tok_rows, share), jnp.bfloat16)],
        8 * tok_rows * width,
    )


def local(
    tokens,
    w_query,
    w_key,
    w_value,
    w_pool_in,
    sink,
    w_pool,
    pool_scale,
    w_out_attn,
    w_out_pool,
    out_gain,
):
    tok_rows = tokens.shape[0]
    tp_count = lax.axis_size("tp")
    tp_here = lax.axis_index("tp")
    seq_len = tok_rows * lax.axis_size("sp")
    key_cols = w_key.shape[1]

    joined = pack_in(w_query, w_key, w_value, w_pool_in)
    weights = gather_sp(joined)
    all_tokens = gather_tp(tokens)

    turned = pack_out(w_out_attn, w_out_pool, tp_count)
    slice_cols, out_rows = turned[0].shape
    mine = jnp.zeros((slice_cols, out_rows * tp_count), tokens.dtype)
    for mask, part in enumerate(turned):
        if mask:
            part = swap(part, "tp", mask)
        mine = lax.dynamic_update_slice_in_dim(mine, part, (tp_here ^ mask) * out_rows, 1)
    out_weights = gather_sp(mine)

    rim = 2 ** (POOL_GROUPS - 1)
    widths = [2 * key_cols, w_query.shape[1], w_pool_in.shape[1]]
    key_value, query, chan, head, tail = project(all_tokens, weights, widths, rim)
    above, below = exchange(head, tail)
    attended = attend(query, key_value, above, below, sink, key_cols, seq_len)
    pooled = pool(chan, above, below, w_pool, pool_scale, seq_len)
    pieces = mix_out(gather_tp(attended), gather_tp(pooled), out_weights)
    pieces = {m: p if m == 0 else swap(p, "tp", m) for m, p in pieces.items()}
    return close(pieces, out_gain, tok_rows, slice_cols)


def solution(mesh):
    return jax.shard_map(
        local,
        mesh=mesh,
        in_specs=(
            P("sp", "tp"),
            P("sp", "tp"),
            P("sp", "tp"),
            P("sp", "tp"),
            P("sp", "tp"),
            P("tp"),
            P("tp", None, None),
            P("tp"),
            P("tp", "sp"),
            P("tp", "sp"),
            P("tp"),
        ),
        out_specs=P("sp", "tp"),
        check_vma=False,
    )
```

```python
import jax
import jax.numpy as jnp
from jax import lax
from jax.experimental import pallas as pl
from jax.experimental.pallas import tpu as pltpu
from jax.sharding import PartitionSpec as P


HEAD_DIM = 64
POOL_GROUPS = 4
WINDOW = 128
TILE = 128
EDGE = 16


epsilon = 1e-05
masked_score = -1e30
direct_limit = 8
kernel_bytes = 16 * 2**20

VMEM = pl.BlockSpec(memory_space=pltpu.VMEM)


def call(body, operands, outs, scratch=(), flops=0, specs=None, limit=kernel_bytes):
    moved = sum(x.size * x.dtype.itemsize for x in operands)
    many = isinstance(outs, list)
    return pl.pallas_call(
        body,
        out_shape=outs,
        in_specs=specs or [VMEM] * len(operands),
        out_specs=[VMEM] * len(outs) if many else VMEM,
        scratch_shapes=list(scratch),
        cost_estimate=pl.CostEstimate(flops=flops, bytes_accessed=moved, transcendentals=0),
        compiler_params=pltpu.CompilerParams(vmem_limit_bytes=limit),
    )(*operands)


def shape(dims, dtype=jnp.bfloat16):
    return jax.ShapeDtypeStruct(dims, dtype)


def at(index, size):
    return pl.ds(pl.multiple_of(index * size, size), size)


def swap(value, axis, mask):
    count = lax.axis_size(axis)
    return lax.ppermute(value, axis, [(i, i ^ mask) for i in range(count)])


def gather_sp(block, relay=False):
    count = lax.axis_size("sp")
    if count > direct_limit or count & (count - 1):
        return {None: lax.all_gather(block, "sp", axis=0, tiled=True)}

    def move(value, pairs):
        return lax.ppermute(value, "sp", pairs)

    beside = [(i, i ^ 1) for i in range(count)]
    near = {0: block}
    if not relay or count != 8:
        for mask in range(2, count, 2):
            near[mask] = swap(block, "sp", mask)
        parts = dict(near)
        for mask, part in near.items():
            parts[mask ^ 1] = move(part, beside)
        return parts

    inner = [i for i in range(count) if i >> 1 in (1, 2)]
    near[2] = swap(block, "sp", 2)
    near[4] = swap(block, "sp", 4)
    near[6] = (move(block, [(i, i ^ 6) for i in inner]), move(near[4], [(i, i ^ 2) for i in inner]))
    parts = dict(near)
    for mask, part in near.items():
        if isinstance(part, tuple):
            parts[mask ^ 1] = (
                move(part[0], [p for p in beside if p[0] in inner]),
                move(part[1], [p for p in beside if p[0] not in inner]),
            )
        else:
            parts[mask ^ 1] = move(part, beside)
    return parts


def flat(parts, masks=None):
    entries = []
    for mask in parts if masks is None else masks:
        part = parts[mask]
        if isinstance(part, tuple):
            entries += [(mask, True, part[0]), (mask, False, part[1])]
        else:
            entries.append((mask, None, part))
    return entries


def choose(inner, action):
    if inner is None:
        action()
        return
    pair = lax.axis_index("sp") >> 1
    pl.when(((pair == 1) | (pair == 2)) == inner)(action)


def gather_tp(block):
    count = lax.axis_size("tp")
    near = {0: block}
    mask = count // 2
    while mask:
        for known, part in list(near.items()):
            near[known ^ mask] = swap(part, "tp", mask)
        mask //= 2
    return near


def exchange(near, far):
    count = lax.axis_size("sp")
    beside = lax.ppermute(near, "sp", [(i, i ^ 1) for i in range(count)])
    ends = [(i, i + 1) for i in range(1, count - 1, 2)]
    beyond = lax.ppermute(far, "sp", ends + [(j, i) for i, j in ends])
    return beside, beyond


def sides(beside, beyond):
    odd = (lax.axis_index("sp") & 1) == 1
    return jnp.where(odd, beside, beyond), jnp.where(odd, beyond, beside)


def place(entries, refs, store):
    here = lax.axis_index("sp")
    for (mask, inner, _), ref in zip(entries, refs):
        rows = ref.shape[0]

        def action(mask=mask, ref=ref, rows=rows):
            if mask is None:
                store[...] = ref[...]
            else:
                store[at(here ^ mask, rows), :] = ref[...]

        choose(inner, action)


def pack_in(w_query, w_key, w_value, w_pool_in):
    rows = w_query.shape[0]
    if rows % 128:
        return jnp.concatenate([w_key, w_value, w_query, w_pool_in], axis=1)

    sizes = [w_key.shape[1], w_value.shape[1], w_query.shape[1], w_pool_in.shape[1]]
    starts = [sum(sizes[:k]) for k in range(5)]

    def body(q_ref, k_ref, v_ref, p_ref, joined_ref, keys, values, sems):
        copies = [
            pltpu.make_async_copy(k_ref, keys, sems.at[0]),
            pltpu.make_async_copy(v_ref, values, sems.at[1]),
            pltpu.make_async_copy(q_ref, joined_ref.at[:, starts[2] : starts[3]], sems.at[2]),
            pltpu.make_async_copy(p_ref, joined_ref.at[:, starts[3] : starts[4]], sems.at[3]),
        ]
        for copy in copies:
            copy.start()
        copies[0].wait()
        copies[1].wait()
        joined_ref[:, : starts[2]] = jnp.concatenate([keys[...].T, values[...].T], axis=1)
        copies[2].wait()
        copies[3].wait()

    return call(
        body,
        [w_query, w_key.T, w_value.T, w_pool_in],
        shape((rows, starts[4])),
        [
            pltpu.VMEM((sizes[0], rows), jnp.bfloat16),
            pltpu.VMEM((sizes[1], rows), jnp.bfloat16),
            pltpu.SemaphoreType.DMA((4,)),
        ],
        specs=[pl.BlockSpec(memory_space=pltpu.HBM)] * 4,
        limit=60 * 2**20,
    )


def pack_out(w_out_attn, w_out_pool, sink, scale, tp_count):
    out_cols = w_out_attn.shape[1]
    depth = w_out_attn.shape[0] + w_out_pool.shape[0]
    width = out_cols // tp_count
    if out_cols % 128 or width % 16:
        whole = jnp.concatenate([w_out_attn, w_out_pool], axis=0).T
        here = lax.axis_index("tp")
        slices = [
            lax.dynamic_slice_in_dim(whole, (here ^ mask) * width, width, 0)
            for mask in range(tp_count)
        ]
        return slices, sink, scale

    def body(a_ref, b_ref, sink_ref, scale_ref, *refs):
        sink_out, scale_out, store = refs[-3:]
        here = lax.axis_index("tp")
        store[...] = jnp.concatenate([a_ref[...].T, b_ref[...].T], axis=1)
        for mask, ref in enumerate(refs[:-3]):
            ref[...] = store[at(here ^ mask, width), :]
        sink_out[...] = sink_ref[...]
        scale_out[...] = scale_ref[...]

    *slices, sink, scale = call(
        body,
        [w_out_attn, w_out_pool, sink, scale],
        [shape((width, depth)) for _ in range(tp_count)]
        + [shape(x.shape, jnp.float32) for x in (sink, scale)],
        [pltpu.VMEM((out_cols, depth), jnp.bfloat16)],
    )
    return slices, sink, scale


def assemble(parts):
    rows, width = parts[0].shape
    if rows % 16:
        here = lax.axis_index("tp")
        whole = jnp.zeros((rows, width * len(parts)), parts[0].dtype)
        for mask, part in enumerate(parts):
            whole = lax.dynamic_update_slice_in_dim(whole, part, (here ^ mask) * width, 1)
        return whole

    def body(*refs):
        here = lax.axis_index("tp")
        for mask, ref in enumerate(refs[:-1]):
            refs[-1][:, at(here ^ mask, width)] = ref[...]

    return call(body, parts, shape((rows, width * len(parts))))


def project(tokens, weights, widths, rim):
    parts = flat(weights)
    masks = list(tokens)
    tok_rows, tok_cols = tokens[0].shape
    wide = sum(widths)
    total = tok_cols * len(masks)
    tile = min(TILE, tok_rows)
    lanes = widths[0]
    pack_rows = WINDOW + rim * (widths[2] // lanes)

    def body(*refs):
        tok_refs = refs[: len(masks)]
        w_refs = refs[len(masks) : len(masks) + len(parts)]
        outs = refs[len(masks) + len(parts) : -3]
        near_ref, far_ref, store = refs[-3:]
        here = lax.axis_index("tp")
        place(parts, w_refs, store)

        def step(i, carry):
            rows = at(i, tile)
            acc = None
            for mask, ref in zip(masks, tok_refs):
                part = jnp.dot(
                    ref[rows, :],
                    store[at(here ^ mask, tok_cols), :],
                    preferred_element_type=jnp.float32,
                )
                acc = part if acc is None else acc + part
            acc = acc.astype(jnp.bfloat16)
            start = 0
            for out, width in zip(outs, widths):
                out[rows, :] = acc[:, start : start + width]
                start += width
            return carry

        lax.fori_loop(0, tok_rows // tile, step, 0)
        odd = (lax.axis_index("sp") & 1) == 1
        for kv_start, rim_start, last in (
            (0, 0, False),
            (tok_rows - WINDOW, tok_rows - rim, True),
        ):
            rows = outs[0][kv_start : kv_start + WINDOW, :]
            edge = outs[2][rim_start : rim_start + rim, :].astype(jnp.float32)
            edge = jnp.concatenate(
                [edge[:, c : c + lanes] for c in range(0, widths[2], lanes)], axis=0
            ).astype(jnp.bfloat16)
            for ref, wanted in ((near_ref, odd != last), (far_ref, odd == last)):
                @pl.when(wanted)
                def _():
                    ref[0:WINDOW, :] = rows
                    ref[WINDOW:pack_rows, :] = edge

    operands = [tokens[m] for m in masks] + [part for *_, part in parts]
    return call(
        body,
        operands,
        [shape((tok_rows, width)) for width in widths] + [shape((pack_rows, lanes))] * 2,
        [pltpu.VMEM((total, wide), jnp.bfloat16)],
        2 * tok_rows * total * wide,
    )


def attend_blocks(work, low, q_ref, store, turned, sink_ref, out_ref, key_cols, inside):
    query_cols = q_ref.shape[1]
    kv_local = key_cols // HEAD_DIM
    group = query_cols // key_cols
    blocks = q_ref.shape[0] // WINDOW
    span = 3 * WINDOW
    root = HEAD_DIM**0.5
    rate = 1.4426950408889634 / root
    for b in sorted({b + k for b in work for k in range(3)}):
        rows = slice(b * WINDOW, (b + 1) * WINDOW)
        turned[:, rows] = store[rows, :].T
    key_row = lax.broadcasted_iota(jnp.int32, (WINDOW, WINDOW), 0)
    query_col = lax.broadcasted_iota(jnp.int32, (WINDOW, WINDOW), 1)
    for index, b in enumerate(work):
        rows = slice(b * WINDOW, (b + 1) * WINDOW)
        target = slice(low + index * WINDOW, low + (index + 1) * WINDOW)
        keep_first = key_row >= query_col
        keep_last = key_row <= query_col
        if b == 0:
            keep_first &= inside[0]
        if b == blocks - 1:
            keep_last &= inside[1]
        query_turned = q_ref[rows, :].T
        pieces = []
        for kv in range(kv_local):
            lane = slice(kv * HEAD_DIM, (kv + 1) * HEAD_DIM)
            keys = store[b * WINDOW : b * WINDOW + span, lane]
            values = turned[
                key_cols + kv * HEAD_DIM : key_cols + (kv + 1) * HEAD_DIM,
                b * WINDOW : b * WINDOW + span,
            ]
            for member in range(group):
                head = kv * group + member
                scores = jnp.dot(
                    keys,
                    query_turned[head * HEAD_DIM : (head + 1) * HEAD_DIM, :],
                    preferred_element_type=jnp.float32,
                )
                scores = jnp.concatenate(
                    [
                        jnp.where(keep_first, scores[:WINDOW], masked_score),
                        scores[WINDOW : 2 * WINDOW],
                        jnp.where(keep_last, scores[2 * WINDOW :], masked_score),
                    ],
                    axis=0,
                )
                sink = sink_ref[:, head : head + 1] * root
                top = jnp.maximum(jnp.max(scores, axis=0, keepdims=True), sink)
                raised = jnp.exp2((scores - top) * rate)
                whole = jnp.sum(raised, axis=0, keepdims=True) + jnp.exp2((sink - top) * rate)
                probs = (raised * (1.0 / whole)).astype(jnp.bfloat16)
                pieces.append(jnp.dot(values, probs, preferred_element_type=jnp.float32))
        out_ref[target, :] = jnp.concatenate(pieces, axis=0).T.astype(jnp.bfloat16)


def pool_rows(cells, start, first_row, count, seq_len, w_ref, scale_ref):
    full, chan_cols = cells.shape
    groups = w_ref.shape[0]
    wide = chan_cols // groups
    position = lax.broadcasted_iota(jnp.int32, (count, 1), 0) + first_row
    outs = []
    for g in range(groups):
        level = lax.axis_index("tp") * groups + g
        cols = slice(g * wide, (g + 1) * wide)
        run = cells[:, cols] + pltpu.roll(cells[:, cols], 1, 0)
        window = run
        for step in range(1, POOL_GROUPS):
            reach = 2 ** (step - 1)
            run = pltpu.roll(run, reach, 0) + pltpu.roll(run, full - reach, 0)
            window = jnp.where(level >= step, run, window)
        half = jnp.left_shift(jnp.int32(1), level)
        width = jnp.minimum(position + half, seq_len) - jnp.maximum(position - half, 0)
        mean = window[start : start + count] / width.astype(jnp.float32)
        spread = (mean - cells[start : start + count, cols]).astype(jnp.bfloat16)
        mapped = jnp.dot(spread, w_ref[g], preferred_element_type=jnp.float32)
        outs.append((mapped * scale_ref[:, cols]).astype(jnp.bfloat16))
    return jnp.concatenate(outs, axis=1)


def hidden_inner(query, key_value, chan, sink, w_pool, pool_scale, key_cols, seq_len):
    tok_rows, query_cols = query.shape
    blocks = tok_rows // WINDOW
    work = list(range(1, blocks - 1))

    def body(q_ref, kv_ref, chan_ref, sink_ref, w_ref, scale_ref, out_ref, store, turned):
        store[WINDOW : WINDOW + tok_rows, :] = kv_ref[...]
        attend_blocks(work, 0, q_ref, store, turned, sink_ref, out_ref, key_cols, None)
        offset = lax.axis_index("sp") * tok_rows
        cells = chan_ref[...].astype(jnp.float32)
        out_ref[len(work) * WINDOW :, :] = pool_rows(
            cells, 0, offset, tok_rows, seq_len, w_ref, scale_ref
        )

    return call(
        body,
        [query, key_value, chan, sink, w_pool, pool_scale],
        shape((len(work) * WINDOW + tok_rows, query_cols)),
        [
            pltpu.VMEM((tok_rows + 2 * WINDOW, 2 * key_cols), jnp.bfloat16),
            pltpu.VMEM((2 * key_cols, tok_rows + 2 * WINDOW), jnp.bfloat16),
        ],
        12 * len(work) * WINDOW * WINDOW * query_cols,
    )


def hidden_outer(query, key_value, chan, halo, sink, w_pool, pool_scale, key_cols, seq_len):
    tok_rows, query_cols = query.shape
    blocks = tok_rows // WINDOW
    chan_cols = chan.shape[1]
    lanes = halo[0].shape[1]
    rim = (halo[0].shape[0] - WINDOW) * lanes // chan_cols
    reach = 2 * EDGE

    def edge(ref):
        rows = ref[WINDOW:, :].astype(jnp.float32)
        return jnp.concatenate(
            [rows[c * rim : (c + 1) * rim] for c in range(chan_cols // lanes)], axis=1
        )

    def body(*refs):
        q_ref, kv_ref, chan_ref, beside_ref, beyond_ref, sink_ref, w_ref, scale_ref = refs[:8]
        out_ref, store, turned = refs[8:]
        offset = lax.axis_index("sp") * tok_rows
        up, down = sides(beside_ref[0:WINDOW, :], beyond_ref[0:WINDOW, :])
        store[0:WINDOW, :] = up
        store[WINDOW : WINDOW + tok_rows, :] = kv_ref[...]
        store[WINDOW + tok_rows :, :] = down
        inside = (offset > 0, offset + tok_rows < seq_len)
        attend_blocks(
            [0, blocks - 1], 0, q_ref, store, turned, sink_ref, out_ref, key_cols, inside
        )
        up, down = sides(edge(beside_ref), edge(beyond_ref))
        first = jnp.concatenate([up, chan_ref[0:reach, :].astype(jnp.float32)], axis=0)
        last = jnp.concatenate([chan_ref[tok_rows - reach :, :].astype(jnp.float32), down], axis=0)
        base = 2 * WINDOW
        out_ref[base : base + EDGE, :] = pool_rows(
            first, rim, offset, EDGE, seq_len, w_ref, scale_ref
        )
        out_ref[base + EDGE :, :] = pool_rows(
            last, reach - EDGE, offset + tok_rows - EDGE, EDGE, seq_len, w_ref, scale_ref
        )

    return call(
        body,
        [query, key_value, chan, *halo, sink, w_pool, pool_scale],
        shape((2 * WINDOW + 2 * EDGE, query_cols)),
        [
            pltpu.VMEM((tok_rows + 2 * WINDOW, 2 * key_cols), jnp.bfloat16),
            pltpu.VMEM((2 * key_cols, tok_rows + 2 * WINDOW), jnp.bfloat16),
        ],
        24 * WINDOW * WINDOW * query_cols,
    )


def hidden_tile(i, tok_rows, inner_ref, outer_ref):
    blocks = tok_rows // WINDOW
    base = (blocks - 2) * WINDOW
    pooled = inner_ref[base + i * WINDOW : base + (i + 1) * WINDOW, :]
    edge = 2 * WINDOW
    if i == 0:
        attended = outer_ref[0:WINDOW, :]
        pooled = jnp.concatenate([outer_ref[edge : edge + EDGE, :], pooled[EDGE:]], axis=0)
    elif i == blocks - 1:
        attended = outer_ref[WINDOW : 2 * WINDOW, :]
        pooled = jnp.concatenate([pooled[:-EDGE], outer_ref[edge + EDGE :, :]], axis=0)
    else:
        attended = inner_ref[(i - 1) * WINDOW : i * WINDOW, :]
    return attended, pooled


def mixed_tile(i, tok_rows, masks, hidden_refs, store):
    n = len(masks)
    here = lax.axis_index("tp")
    contract = (((1,), (1,)), ((), ()))
    mix = None
    for mask, inner_ref, outer_ref in zip(masks, hidden_refs[:n], hidden_refs[n:]):
        partial = None
        wide = inner_ref.shape[1]
        base = (here ^ mask) * (2 * wide)
        for k, rows in enumerate(hidden_tile(i, tok_rows, inner_ref, outer_ref)):
            term = lax.dot_general(
                rows,
                store[:, pl.ds(pl.multiple_of(base + k * wide, wide), wide)],
                contract,
                preferred_element_type=jnp.float32,
            )
            partial = term if partial is None else partial + term
        partial = partial.astype(jnp.bfloat16).astype(jnp.float32)
        mix = partial if mix is None else mix + partial
    return mix


def folded(values):
    lanes = sum(values[:, k : k + 128] for k in range(0, values.shape[1], 128))
    return jnp.sum(lanes.T, axis=0, keepdims=True)


def three_terms(total, square):
    terms = []
    for rest in (total, square):
        for _ in range(3):
            term = rest.astype(jnp.bfloat16).astype(jnp.float32)
            terms.append(term)
            rest = rest - term
    terms.append(jnp.zeros((2, total.shape[1]), jnp.float32))
    return jnp.concatenate(terms, axis=0)


def mix_out(inner, outer, weights, tok_rows):
    masks = list(inner)
    n = len(masks)
    parts = flat(weights)
    depth = 2 * inner[0].shape[1]
    cols = sum(part.shape[0] for _, side, part in parts if side is not False)
    share = cols // n
    tiles = tok_rows // WINDOW

    def body(*refs):
        hidden_refs = refs[: 2 * n]
        w_refs = refs[2 * n : 2 * n + len(parts)]
        piece_refs = refs[2 * n + len(parts) : 3 * n + len(parts)]
        sums, store = refs[-2:]
        here = lax.axis_index("tp")
        place(parts, w_refs, store)
        for i in range(tiles):
            rows = slice(i * WINDOW, (i + 1) * WINDOW)
            mix = mixed_tile(i, tok_rows, masks, hidden_refs, store)
            sums[8 * i : 8 * (i + 1), :] = three_terms(folded(mix), folded(mix * mix))
            whole = mix.astype(jnp.bfloat16)
            for k in range(n):
                part = whole[:, k * share : (k + 1) * share]
                for mask, ref in zip(masks, piece_refs):
                    @pl.when((here ^ mask) == k)
                    def _():
                        ref[rows, :] = part

        for ref in piece_refs:
            ref[tok_rows:, :] = sums[...].astype(jnp.bfloat16)

    extra = 8 * tiles
    results = call(
        body,
        [*inner.values(), *outer.values()] + [part for *_, part in parts],
        [shape((tok_rows + extra, share)) for _ in masks],
        [pltpu.VMEM((extra, WINDOW), jnp.float32), pltpu.VMEM((cols, depth * n), jnp.bfloat16)],
        2 * tok_rows * depth * n * cols,
    )
    return dict(zip(masks, results))


def mix_step(inner, outer, weights, tok_rows, groups, earlier=None):
    masks = list(inner)
    n = len(masks)
    depth = 2 * inner[0].shape[1]
    blocks = flat(weights, [2 * g + side for g in groups for side in (0, 1)])
    half = weights[0].shape[0]
    share = 2 * half
    cols = share * len(groups)
    tiles = tok_rows // WINDOW
    held = [] if earlier is None else list(earlier)

    def body(*refs):
        hidden_refs = refs[: 2 * n]
        w_refs = refs[2 * n : 2 * n + len(blocks)]
        held_refs = refs[2 * n + len(blocks) : 2 * n + len(blocks) + len(held)]
        store = refs[-1]
        here = lax.axis_index("tp")
        spot = lax.axis_index("sp")
        for (block, side, _), ref in zip(blocks, w_refs):
            row = (groups.index(block // 2) * 2 + ((spot ^ block) & 1)) * half

            def action(row=row, ref=ref):
                store[pl.ds(pl.multiple_of(row, half), half), :] = ref[...]

            choose(side, action)

        if earlier is None:
            outs = refs[-len(groups) - 2 : -2]
            sums = refs[-2]
        else:
            outs = refs[-n - 3 : -3]
            last, sums = refs[-3:-1]
        for i in range(tiles):
            rows = slice(i * WINDOW, (i + 1) * WINDOW)
            mix = mixed_tile(i, tok_rows, masks, hidden_refs, store)
            total, square = folded(mix), folded(mix * mix)
            whole = mix.astype(jnp.bfloat16)
            if earlier is None:
                sums[8 * i : 8 * i + 1, :] = total
                sums[8 * i + 1 : 8 * i + 2, :] = square
                for k, out in enumerate(outs):
                    out[rows, :] = whole[:, k * share : (k + 1) * share]
            else:
                last[rows, :] = whole
                sums[8 * i : 8 * (i + 1), :] = three_terms(
                    total + held_refs[-1][8 * i : 8 * i + 1, :],
                    square + held_refs[-1][8 * i + 1 : 8 * i + 2, :],
                )
        if earlier is None:
            return
        sources = [*held_refs[:-1], last]
        for mask, out in zip(masks, outs):
            out[tok_rows:, :] = sums[...].astype(jnp.bfloat16)
            distance = (spot >> 1) ^ here ^ mask
            for k, source in enumerate(sources):
                @pl.when(distance == k)
                def _():
                    out[0:tok_rows, :] = source[...]

    store = pltpu.VMEM((cols, depth * n), jnp.bfloat16)
    if earlier is None:
        outs = [shape((tok_rows, share)) for _ in groups]
        outs.append(shape((8 * tiles, WINDOW), jnp.float32))
        scratch = [store]
    else:
        outs = [shape((tok_rows + 8 * tiles, share)) for _ in masks]
        scratch = [
            pltpu.VMEM((tok_rows, share), jnp.bfloat16),
            pltpu.VMEM((8 * tiles, WINDOW), jnp.float32),
            store,
        ]
    return call(
        body,
        [*inner.values(), *outer.values()] + [part for *_, part in blocks] + held,
        outs,
        scratch,
        2 * tok_rows * depth * n * cols,
    )


def mix_staged(inner, outer, weights, tok_rows):
    pairs = len(weights) // 2
    early = mix_step(inner, outer, weights, tok_rows, list(range(pairs - 1)))
    late = mix_step(inner, outer, weights, tok_rows, [pairs - 1], early)
    return dict(zip(inner, late))


def close(pieces, out_gain, tok_rows, slice_cols):
    masks = list(pieces)
    held, share = pieces[0].shape
    width = out_gain.shape[0]
    model_width = width * len(masks)
    tile = min(TILE, tok_rows)

    def moments(sums):
        mean = sum(sums[k : k + 1] for k in range(3)) / model_width
        square = sum(sums[k : k + 1] for k in range(3, 6)) / model_width
        return mean, lax.rsqrt(square - mean * mean + epsilon)

    if slice_cols % 64:
        here = lax.axis_index("tp")
        stacked = jnp.zeros((len(masks), held, share), jnp.bfloat16)
        for mask, part in pieces.items():
            stacked = lax.dynamic_update_slice_in_dim(stacked, part[None], here ^ mask, 0)
        sums = jnp.sum(stacked[:, tok_rows:].astype(jnp.float32), axis=0)
        mean, scale = moments(sums.reshape(-1, 8, tile).transpose(1, 0, 2).reshape(8, -1))
        grid = stacked[:, :tok_rows].reshape(len(masks), tok_rows, -1, slice_cols)
        mixed = grid.transpose(1, 2, 0, 3).reshape(tok_rows, width).astype(jnp.float32)
        return ((mixed - mean.T) * scale.T * out_gain).astype(jnp.bfloat16)

    def body(*refs):
        n = len(masks)
        piece_refs = refs[:n]
        gain_ref, out_ref, store = refs[n:]
        here = lax.axis_index("tp")
        total = None
        for mask, ref in zip(masks, piece_refs):
            store[here ^ mask] = ref[0:tok_rows, :]
            sums = ref[tok_rows:, :].astype(jnp.float32)
            total = sums if total is None else total + sums
        for i in range(tok_rows // tile):
            rows = slice(i * tile, (i + 1) * tile)
            mean, scale = moments(total[8 * i : 8 * (i + 1)])
            mean = jnp.broadcast_to(mean, (128, tile)).T[:, 0:1]
            scale = jnp.broadcast_to(scale, (128, tile)).T[:, 0:1]
            parts = []
            for block in range(share // slice_cols):
                cols = slice(block * slice_cols, (block + 1) * slice_cols)
                parts += [store[k, rows, cols] for k in range(n)]
            mixed = jnp.concatenate(parts, axis=1).astype(jnp.float32)
            out_ref[rows, :] = ((mixed - mean) * scale * gain_ref[...]).astype(jnp.bfloat16)

    return call(
        body,
        [pieces[m] for m in masks] + [out_gain.reshape(1, width)],
        shape((tok_rows, width)),
        [pltpu.VMEM((len(masks), tok_rows, share), jnp.bfloat16)],
        8 * tok_rows * width,
    )


def local(
    tokens,
    w_query,
    w_key,
    w_value,
    w_pool_in,
    sink,
    w_pool,
    pool_scale,
    w_out_attn,
    w_out_pool,
    out_gain,
):
    tok_rows = tokens.shape[0]
    tp_count = lax.axis_size("tp")
    seq_len = tok_rows * lax.axis_size("sp")
    key_cols = w_key.shape[1]

    joined = pack_in(w_query, w_key, w_value, w_pool_in)
    weights = gather_sp(joined)
    all_tokens = gather_tp(tokens)

    turned, sink, pool_scale = pack_out(
        w_out_attn, w_out_pool, sink.reshape(1, -1), pool_scale.reshape(1, -1), tp_count
    )
    slice_cols, _ = turned[0].shape
    parts = [turned[0]] + [swap(turned[mask], "tp", mask) for mask in range(1, tp_count)]
    mine = assemble(parts)
    out_weights = gather_sp(mine, True)

    rim = 2 ** (POOL_GROUPS - 1)
    widths = [2 * key_cols, w_query.shape[1], w_pool_in.shape[1]]
    key_value, query, chan, near, far = project(all_tokens, weights, widths, rim)
    halo = exchange(near, far)
    small = (sink, w_pool, pool_scale, key_cols, seq_len)
    inner = gather_tp(hidden_inner(query, key_value, chan, *small))
    outer = gather_tp(hidden_outer(query, key_value, chan, halo, *small))
    mix = mix_staged if len(out_weights) == 2 * tp_count else mix_out
    pieces = mix(inner, outer, out_weights, tok_rows)
    pieces = {m: p if m == 0 else swap(p, "tp", m) for m, p in pieces.items()}
    return close(pieces, out_gain, tok_rows, slice_cols)


def solution(mesh):
    return jax.shard_map(
        local,
        mesh=mesh,
        in_specs=(
            P("sp", "tp"),
            P("sp", "tp"),
            P("sp", "tp"),
            P("sp", "tp"),
            P("sp", "tp"),
            P("tp"),
            P("tp", None, None),
            P("tp"),
            P("tp", "sp"),
            P("tp", "sp"),
            P("tp"),
        ),
        out_specs=P("sp", "tp"),
        check_vma=False,
    )
```

```python
import jax
import jax.numpy as jnp
from jax import lax
from jax.experimental import pallas as pl
from jax.experimental.pallas import tpu as pltpu
from jax.sharding import PartitionSpec as P


HEAD_DIM = 64
POOL_GROUPS = 4
WINDOW = 128
TILE = 128
EDGE = 16


epsilon = 1e-05
masked_score = -1e30
direct_limit = 8
kernel_bytes = 16 * 2**20

VMEM = pl.BlockSpec(memory_space=pltpu.VMEM)


def call(body, operands, outs, scratch=(), flops=0, specs=None, limit=kernel_bytes):
    moved = sum(x.size * x.dtype.itemsize for x in operands)
    many = isinstance(outs, list)
    return pl.pallas_call(
        body,
        out_shape=outs,
        in_specs=specs or [VMEM] * len(operands),
        out_specs=[VMEM] * len(outs) if many else VMEM,
        scratch_shapes=list(scratch),
        cost_estimate=pl.CostEstimate(flops=flops, bytes_accessed=moved, transcendentals=0),
        compiler_params=pltpu.CompilerParams(vmem_limit_bytes=limit),
    )(*operands)


def shape(dims, dtype=jnp.bfloat16):
    return jax.ShapeDtypeStruct(dims, dtype)


def at(index, size):
    return pl.ds(pl.multiple_of(index * size, size), size)


def swap(value, axis, mask):
    count = lax.axis_size(axis)
    return lax.ppermute(value, axis, [(i, i ^ mask) for i in range(count)])


def gather_sp(block, relay=False):
    count = lax.axis_size("sp")
    if count > direct_limit or count & (count - 1):
        return {None: lax.all_gather(block, "sp", axis=0, tiled=True)}

    def move(value, pairs):
        return lax.ppermute(value, "sp", pairs)

    beside = [(i, i ^ 1) for i in range(count)]
    near = {0: block}
    if not relay or count != 8:
        for mask in range(2, count, 2):
            near[mask] = swap(block, "sp", mask)
        parts = dict(near)
        for mask, part in near.items():
            if mask == 2:
                parts[3] = swap(parts[1], "sp", 2)
            else:
                parts[mask ^ 1] = move(part, beside)
        return parts

    inner = [i for i in range(count) if i >> 1 in (1, 2)]
    near[2] = swap(block, "sp", 2)
    near[4] = swap(block, "sp", 4)
    near[6] = (move(block, [(i, i ^ 6) for i in inner]), move(near[4], [(i, i ^ 2) for i in inner]))
    parts = dict(near)
    for mask, part in near.items():
        if isinstance(part, tuple):
            parts[mask ^ 1] = (
                move(part[0], [p for p in beside if p[0] in inner]),
                move(part[1], [p for p in beside if p[0] not in inner]),
            )
        else:
            parts[mask ^ 1] = move(part, beside)
    return parts


def flat(parts, masks=None):
    entries = []
    for mask in parts if masks is None else masks:
        part = parts[mask]
        if isinstance(part, tuple):
            entries += [(mask, True, part[0]), (mask, False, part[1])]
        else:
            entries.append((mask, None, part))
    return entries


def choose(inner, action):
    if inner is None:
        action()
        return
    pair = lax.axis_index("sp") >> 1
    pl.when(((pair == 1) | (pair == 2)) == inner)(action)


def gather_tp(block):
    count = lax.axis_size("tp")
    near = {0: block}
    mask = count // 2
    while mask:
        for known, part in list(near.items()):
            near[known ^ mask] = swap(part, "tp", mask)
        mask //= 2
    return near


def exchange(near, far):
    count = lax.axis_size("sp")
    beside = lax.ppermute(near, "sp", [(i, i ^ 1) for i in range(count)])
    ends = [(i, i + 1) for i in range(1, count - 1, 2)]
    beyond = lax.ppermute(far, "sp", ends + [(j, i) for i, j in ends])
    return beside, beyond


def sides(beside, beyond):
    odd = (lax.axis_index("sp") & 1) == 1
    return jnp.where(odd, beside, beyond), jnp.where(odd, beyond, beside)


def place(entries, refs, store):
    here = lax.axis_index("sp")
    for (mask, inner, _), ref in zip(entries, refs):
        rows = ref.shape[0]

        def action(mask=mask, ref=ref, rows=rows):
            if mask is None:
                store[...] = ref[...]
            else:
                store[at(here ^ mask, rows), :] = ref[...]

        choose(inner, action)


def pack_in(w_query, w_key, w_value, w_pool_in):
    rows = w_query.shape[0]
    if rows % 128:
        return jnp.concatenate([w_key, w_value, w_query, w_pool_in], axis=1)

    sizes = [w_key.shape[1], w_value.shape[1], w_query.shape[1], w_pool_in.shape[1]]
    starts = [sum(sizes[:k]) for k in range(5)]

    def body(q_ref, k_ref, v_ref, p_ref, joined_ref, keys, values, sems):
        copies = [
            pltpu.make_async_copy(k_ref, keys, sems.at[0]),
            pltpu.make_async_copy(v_ref, values, sems.at[1]),
            pltpu.make_async_copy(q_ref, joined_ref.at[:, starts[2] : starts[3]], sems.at[2]),
            pltpu.make_async_copy(p_ref, joined_ref.at[:, starts[3] : starts[4]], sems.at[3]),
        ]
        for copy in copies:
            copy.start()
        copies[0].wait()
        copies[1].wait()
        joined_ref[:, : starts[2]] = jnp.concatenate([keys[...].T, values[...].T], axis=1)
        copies[2].wait()
        copies[3].wait()

    return call(
        body,
        [w_query, w_key.T, w_value.T, w_pool_in],
        shape((rows, starts[4])),
        [
            pltpu.VMEM((sizes[0], rows), jnp.bfloat16),
            pltpu.VMEM((sizes[1], rows), jnp.bfloat16),
            pltpu.SemaphoreType.DMA((4,)),
        ],
        specs=[pl.BlockSpec(memory_space=pltpu.HBM)] * 4,
        limit=60 * 2**20,
    )


def pack_out(w_out_attn, w_out_pool, tp_count):
    out_cols = w_out_attn.shape[1]
    depth = w_out_attn.shape[0] + w_out_pool.shape[0]
    width = out_cols // tp_count
    if out_cols % 128 or width % 16:
        whole = jnp.concatenate([w_out_attn, w_out_pool], axis=0).T
        here = lax.axis_index("tp")
        return [
            lax.dynamic_slice_in_dim(whole, (here ^ mask) * width, width, 0)
            for mask in range(tp_count)
        ]

    def body(a_ref, b_ref, *refs):
        store = refs[-1]
        here = lax.axis_index("tp")
        store[...] = jnp.concatenate([a_ref[...].T, b_ref[...].T], axis=1)
        for mask, ref in enumerate(refs[:-1]):
            ref[...] = store[at(here ^ mask, width), :]

    return call(
        body,
        [w_out_attn, w_out_pool],
        [shape((width, depth)) for _ in range(tp_count)],
        [pltpu.VMEM((out_cols, depth), jnp.bfloat16)],
    )


def assemble(parts, others):
    rows, width = parts[0].shape
    if rows % 16:
        here = lax.axis_index("tp")
        whole = jnp.zeros((rows, width * len(parts)), parts[0].dtype)
        for mask, part in enumerate(parts):
            whole = lax.dynamic_update_slice_in_dim(whole, part, (here ^ mask) * width, 1)
        return [whole, *others]

    def body(*refs):
        here = lax.axis_index("tp")
        whole = refs[len(parts) + len(others)]
        for mask, ref in enumerate(refs[: len(parts)]):
            whole[:, at(here ^ mask, width)] = ref[...]
        for source, target in zip(refs[len(parts) :], refs[len(parts) + len(others) + 1 :]):
            target[...] = source[...]

    return call(
        body,
        [*parts, *others],
        [shape((rows, width * len(parts)))] + [shape(x.shape, x.dtype) for x in others],
    )


def write_projected(acc, rows, outs, widths):
    rounded = acc.astype(jnp.bfloat16)
    start = 0
    for out, width in zip(outs, widths):
        out[rows, :] = rounded[:, start : start + width]
        start += width


def write_halo(outs, near_ref, far_ref, widths, rim):
    tok_rows = outs[0].shape[0]
    lanes = widths[0]
    odd = (lax.axis_index("sp") & 1) == 1
    for kv_start, rim_start, last in (
        (0, 0, False),
        (tok_rows - WINDOW, tok_rows - rim, True),
    ):
        rows = outs[0][kv_start : kv_start + WINDOW, :]
        edge = outs[2][rim_start : rim_start + rim, :].astype(jnp.float32)
        edge = jnp.concatenate(
            [edge[:, c : c + lanes] for c in range(0, widths[2], lanes)], axis=0
        ).astype(jnp.bfloat16)
        for ref, wanted in ((near_ref, odd != last), (far_ref, odd == last)):
            @pl.when(wanted)
            def _():
                ref[0:WINDOW, :] = rows
                ref[WINDOW:, :] = edge


def projected_shapes(tok_rows, widths, rim):
    pack = shape((WINDOW + rim * (widths[2] // widths[0]), widths[0]))
    return [shape((tok_rows, width)) for width in widths] + [pack, pack]


def project(tokens, weights, widths, rim):
    parts = flat(weights)
    masks = list(tokens)
    tok_rows, tok_cols = tokens[0].shape
    total = tok_cols * len(masks)

    def body(*refs):
        tok_refs = refs[: len(masks)]
        w_refs = refs[len(masks) : len(masks) + len(parts)]
        outs = refs[len(masks) + len(parts) : -3]
        near_ref, far_ref, store = refs[-3:]
        here = lax.axis_index("tp")
        place(parts, w_refs, store)
        for i in range(tok_rows // TILE):
            rows = slice(i * TILE, (i + 1) * TILE)
            acc = None
            for mask, ref in zip(masks, tok_refs):
                part = jnp.dot(
                    ref[rows, :],
                    store[at(here ^ mask, tok_cols), :],
                    preferred_element_type=jnp.float32,
                )
                acc = part if acc is None else acc + part
            write_projected(acc, rows, outs, widths)
        write_halo(outs, near_ref, far_ref, widths, rim)

    return call(
        body,
        [tokens[m] for m in masks] + [part for *_, part in parts],
        projected_shapes(tok_rows, widths, rim),
        [pltpu.VMEM((total, sum(widths)), jnp.bfloat16)],
        2 * tok_rows * total * sum(widths),
    )


def project_step(tokens, weights, widths, rim, groups, last, earlier=None):
    parts = flat(weights, [2 * g + side for g in groups for side in (0, 1)])
    masks = list(tokens)
    tok_rows, tok_cols = tokens[0].shape
    half = tok_cols // 2
    wide = sum(widths)
    sources = [tokens[m] for m in masks] if earlier is None else [earlier[1]]
    held = [] if earlier is None else [earlier[0]]

    def body(*refs):
        tok_refs = refs[: len(sources)]
        w_refs = refs[len(sources) : len(sources) + len(parts)]
        rest = refs[len(sources) + len(parts) :]
        store = rest[-1]
        here = lax.axis_index("tp")
        spot = lax.axis_index("sp")
        if earlier is None:
            own = rest[-2]
            for group in [*groups, last]:
                distance = (spot >> 1) ^ here ^ group
                for mask, ref in zip(masks, tok_refs):
                    @pl.when(distance == mask)
                    def _():
                        if group == last:
                            rest[1][...] = ref[...]
                        else:
                            own[groups.index(group)] = ref[...]

        for (block, side, _), ref in zip(parts, w_refs):
            row = (groups.index(block // 2) * 2 + ((spot ^ block) & 1)) * half

            def action(row=row, ref=ref):
                store[pl.ds(pl.multiple_of(row, half), half), :] = ref[...]

            choose(side, action)
        for i in range(tok_rows // TILE):
            rows = slice(i * TILE, (i + 1) * TILE)
            acc = None if earlier is None else rest[0][rows, :]
            for index in range(len(groups)):
                part = jnp.dot(
                    own[index, rows, :] if earlier is None else tok_refs[0][rows, :],
                    store[index * tok_cols : (index + 1) * tok_cols, :],
                    preferred_element_type=jnp.float32,
                )
                acc = part if acc is None else acc + part
            if earlier is None:
                rest[0][rows, :] = acc
            else:
                write_projected(acc, rows, rest[1:4], widths)
        if earlier is not None:
            write_halo(rest[1:4], rest[4], rest[5], widths, rim)

    early_scratch = [pltpu.VMEM((len(groups), tok_rows, tok_cols), jnp.bfloat16)]
    return call(
        body,
        sources + [part for *_, part in parts] + held,
        [shape((tok_rows, wide), jnp.float32), shape((tok_rows, tok_cols))]
        if earlier is None
        else projected_shapes(tok_rows, widths, rim),
        (early_scratch if earlier is None else [])
        + [pltpu.VMEM((len(groups) * tok_cols, wide), jnp.bfloat16)],
        2 * tok_rows * len(groups) * tok_cols * wide,
    )


def project_staged(tokens, weights, widths, rim):
    pairs = len(weights) // 2
    last = pairs // 2
    early = [g for g in range(pairs) if g != last]
    sums = project_step(tokens, weights, widths, rim, early, last)
    return project_step(tokens, weights, widths, rim, [last], last, sums)


def attend_blocks(work, low, q_ref, store, turned, sink_ref, out_ref, key_cols, inside):
    query_cols = q_ref.shape[1]
    kv_local = key_cols // HEAD_DIM
    group = query_cols // key_cols
    blocks = q_ref.shape[0] // WINDOW
    span = 3 * WINDOW
    root = HEAD_DIM**0.5
    rate = 1.4426950408889634 / root
    for b in sorted({b + k for b in work for k in range(3)}):
        rows = slice(b * WINDOW, (b + 1) * WINDOW)
        turned[:, rows] = store[rows, :].T
    key_row = lax.broadcasted_iota(jnp.int32, (WINDOW, WINDOW), 0)
    query_col = lax.broadcasted_iota(jnp.int32, (WINDOW, WINDOW), 1)
    for index, b in enumerate(work):
        rows = slice(b * WINDOW, (b + 1) * WINDOW)
        target = slice(low + index * WINDOW, low + (index + 1) * WINDOW)
        keep_first = key_row >= query_col
        keep_last = key_row <= query_col
        if b == 0:
            keep_first &= inside[0]
        if b == blocks - 1:
            keep_last &= inside[1]
        query_turned = q_ref[rows, :].T
        pieces = []
        for kv in range(kv_local):
            lane = slice(kv * HEAD_DIM, (kv + 1) * HEAD_DIM)
            keys = store[b * WINDOW : b * WINDOW + span, lane]
            values = turned[
                key_cols + kv * HEAD_DIM : key_cols + (kv + 1) * HEAD_DIM,
                b * WINDOW : b * WINDOW + span,
            ]
            for member in range(group):
                head = kv * group + member
                scores = jnp.dot(
                    keys,
                    query_turned[head * HEAD_DIM : (head + 1) * HEAD_DIM, :],
                    preferred_element_type=jnp.float32,
                )
                scores = jnp.concatenate(
                    [
                        jnp.where(keep_first, scores[:WINDOW], masked_score),
                        scores[WINDOW : 2 * WINDOW],
                        jnp.where(keep_last, scores[2 * WINDOW :], masked_score),
                    ],
                    axis=0,
                )
                sink = sink_ref[:, head : head + 1] * root
                top = jnp.maximum(jnp.max(scores, axis=0, keepdims=True), sink)
                raised = jnp.exp2((scores - top) * rate)
                whole = jnp.sum(raised, axis=0, keepdims=True) + jnp.exp2((sink - top) * rate)
                probs = (raised * (1.0 / whole)).astype(jnp.bfloat16)
                pieces.append(jnp.dot(values, probs, preferred_element_type=jnp.float32))
        out_ref[target, :] = jnp.concatenate(pieces, axis=0).T.astype(jnp.bfloat16)


def pool_rows(cells, start, first_row, count, seq_len, w_ref, scale_ref):
    full, chan_cols = cells.shape
    groups = w_ref.shape[0]
    wide = chan_cols // groups
    position = lax.broadcasted_iota(jnp.int32, (count, 1), 0) + first_row
    outs = []
    for g in range(groups):
        level = lax.axis_index("tp") * groups + g
        cols = slice(g * wide, (g + 1) * wide)
        run = cells[:, cols] + pltpu.roll(cells[:, cols], 1, 0)
        window = run
        for step in range(1, POOL_GROUPS):
            reach = 2 ** (step - 1)
            run = pltpu.roll(run, reach, 0) + pltpu.roll(run, full - reach, 0)
            window = jnp.where(level >= step, run, window)
        half = jnp.left_shift(jnp.int32(1), level)
        width = jnp.minimum(position + half, seq_len) - jnp.maximum(position - half, 0)
        mean = window[start : start + count] / width.astype(jnp.float32)
        spread = (mean - cells[start : start + count, cols]).astype(jnp.bfloat16)
        mapped = jnp.dot(spread, w_ref[g], preferred_element_type=jnp.float32)
        outs.append((mapped * scale_ref[:, cols]).astype(jnp.bfloat16))
    return jnp.concatenate(outs, axis=1)


def hidden_inner(query, key_value, chan, sink, w_pool, pool_scale, key_cols, seq_len):
    tok_rows, query_cols = query.shape
    blocks = tok_rows // WINDOW
    work = list(range(1, blocks - 1))

    def body(q_ref, kv_ref, chan_ref, sink_ref, w_ref, scale_ref, out_ref, store, turned):
        store[WINDOW : WINDOW + tok_rows, :] = kv_ref[...]
        attend_blocks(work, 0, q_ref, store, turned, sink_ref, out_ref, key_cols, None)
        offset = lax.axis_index("sp") * tok_rows
        cells = chan_ref[...].astype(jnp.float32)
        out_ref[len(work) * WINDOW :, :] = pool_rows(
            cells, 0, offset, tok_rows, seq_len, w_ref, scale_ref
        )

    return call(
        body,
        [query, key_value, chan, sink, w_pool, pool_scale],
        shape((len(work) * WINDOW + tok_rows, query_cols)),
        [
            pltpu.VMEM((tok_rows + 2 * WINDOW, 2 * key_cols), jnp.bfloat16),
            pltpu.VMEM((2 * key_cols, tok_rows + 2 * WINDOW), jnp.bfloat16),
        ],
        12 * len(work) * WINDOW * WINDOW * query_cols,
    )


def hidden_outer(query, key_value, chan, halo, sink, w_pool, pool_scale, key_cols, seq_len):
    tok_rows, query_cols = query.shape
    blocks = tok_rows // WINDOW
    chan_cols = chan.shape[1]
    lanes = halo[0].shape[1]
    rim = (halo[0].shape[0] - WINDOW) * lanes // chan_cols
    reach = 2 * EDGE

    def edge(ref):
        rows = ref[WINDOW:, :].astype(jnp.float32)
        return jnp.concatenate(
            [rows[c * rim : (c + 1) * rim] for c in range(chan_cols // lanes)], axis=1
        )

    def body(*refs):
        q_ref, kv_ref, chan_ref, beside_ref, beyond_ref, sink_ref, w_ref, scale_ref = refs[:8]
        out_ref, store, turned = refs[8:]
        offset = lax.axis_index("sp") * tok_rows
        up, down = sides(beside_ref[0:WINDOW, :], beyond_ref[0:WINDOW, :])
        store[0:WINDOW, :] = up
        store[WINDOW : WINDOW + tok_rows, :] = kv_ref[...]
        store[WINDOW + tok_rows :, :] = down
        inside = (offset > 0, offset + tok_rows < seq_len)
        attend_blocks(
            [0, blocks - 1], 0, q_ref, store, turned, sink_ref, out_ref, key_cols, inside
        )
        up, down = sides(edge(beside_ref), edge(beyond_ref))
        first = jnp.concatenate([up, chan_ref[0:reach, :].astype(jnp.float32)], axis=0)
        last = jnp.concatenate([chan_ref[tok_rows - reach :, :].astype(jnp.float32), down], axis=0)
        base = 2 * WINDOW
        out_ref[base : base + EDGE, :] = pool_rows(
            first, rim, offset, EDGE, seq_len, w_ref, scale_ref
        )
        out_ref[base + EDGE :, :] = pool_rows(
            last, reach - EDGE, offset + tok_rows - EDGE, EDGE, seq_len, w_ref, scale_ref
        )

    return call(
        body,
        [query, key_value, chan, *halo, sink, w_pool, pool_scale],
        shape((2 * WINDOW + 2 * EDGE, query_cols)),
        [
            pltpu.VMEM((tok_rows + 2 * WINDOW, 2 * key_cols), jnp.bfloat16),
            pltpu.VMEM((2 * key_cols, tok_rows + 2 * WINDOW), jnp.bfloat16),
        ],
        24 * WINDOW * WINDOW * query_cols,
    )


def hidden_tile(i, tok_rows, inner_ref, outer_ref):
    blocks = tok_rows // WINDOW
    base = (blocks - 2) * WINDOW
    pooled = inner_ref[base + i * WINDOW : base + (i + 1) * WINDOW, :]
    edge = 2 * WINDOW
    if i == 0:
        attended = outer_ref[0:WINDOW, :]
        pooled = jnp.concatenate([outer_ref[edge : edge + EDGE, :], pooled[EDGE:]], axis=0)
    elif i == blocks - 1:
        attended = outer_ref[WINDOW : 2 * WINDOW, :]
        pooled = jnp.concatenate([pooled[:-EDGE], outer_ref[edge + EDGE :, :]], axis=0)
    else:
        attended = inner_ref[(i - 1) * WINDOW : i * WINDOW, :]
    return attended, pooled


def mixed_tile(i, tok_rows, masks, hidden_refs, store):
    n = len(masks)
    here = lax.axis_index("tp")
    contract = (((1,), (1,)), ((), ()))
    mix = None
    for mask, inner_ref, outer_ref in zip(masks, hidden_refs[:n], hidden_refs[n:]):
        partial = None
        wide = inner_ref.shape[1]
        base = (here ^ mask) * (2 * wide)
        for k, rows in enumerate(hidden_tile(i, tok_rows, inner_ref, outer_ref)):
            term = lax.dot_general(
                rows,
                store[:, pl.ds(pl.multiple_of(base + k * wide, wide), wide)],
                contract,
                preferred_element_type=jnp.float32,
            )
            partial = term if partial is None else partial + term
        partial = partial.astype(jnp.bfloat16).astype(jnp.float32)
        mix = partial if mix is None else mix + partial
    return mix


def folded(values):
    lanes = sum(values[:, k : k + 128] for k in range(0, values.shape[1], 128))
    return jnp.sum(lanes.T, axis=0, keepdims=True)


def three_terms(total, square):
    terms = []
    for rest in (total, square):
        for _ in range(3):
            term = rest.astype(jnp.bfloat16).astype(jnp.float32)
            terms.append(term)
            rest = rest - term
    terms.append(jnp.zeros((2, total.shape[1]), jnp.float32))
    return jnp.concatenate(terms, axis=0)


def mix_out(inner, outer, weights, tok_rows):
    masks = list(inner)
    n = len(masks)
    parts = flat(weights)
    depth = 2 * inner[0].shape[1]
    cols = sum(part.shape[0] for _, side, part in parts if side is not False)
    share = cols // n
    tiles = tok_rows // WINDOW

    def body(*refs):
        hidden_refs = refs[: 2 * n]
        w_refs = refs[2 * n : 2 * n + len(parts)]
        piece_refs = refs[2 * n + len(parts) : 3 * n + len(parts)]
        sums, store = refs[-2:]
        here = lax.axis_index("tp")
        place(parts, w_refs, store)
        for i in range(tiles):
            rows = slice(i * WINDOW, (i + 1) * WINDOW)
            mix = mixed_tile(i, tok_rows, masks, hidden_refs, store)
            sums[8 * i : 8 * (i + 1), :] = three_terms(folded(mix), folded(mix * mix))
            whole = mix.astype(jnp.bfloat16)
            for k in range(n):
                part = whole[:, k * share : (k + 1) * share]
                for mask, ref in zip(masks, piece_refs):
                    @pl.when((here ^ mask) == k)
                    def _():
                        ref[rows, :] = part

        for ref in piece_refs:
            ref[tok_rows:, :] = sums[...].astype(jnp.bfloat16)

    extra = 8 * tiles
    results = call(
        body,
        [*inner.values(), *outer.values()] + [part for *_, part in parts],
        [shape((tok_rows + extra, share)) for _ in masks],
        [pltpu.VMEM((extra, WINDOW), jnp.float32), pltpu.VMEM((cols, depth * n), jnp.bfloat16)],
        2 * tok_rows * depth * n * cols,
    )
    return dict(zip(masks, results))


def mix_step(inner, outer, weights, tok_rows, groups, earlier=None):
    masks = list(inner)
    n = len(masks)
    depth = 2 * inner[0].shape[1]
    blocks = flat(weights, [2 * g + side for g in groups for side in (0, 1)])
    half = weights[0].shape[0]
    share = 2 * half
    cols = share * len(groups)
    tiles = tok_rows // WINDOW
    held = [] if earlier is None else list(earlier)

    def body(*refs):
        hidden_refs = refs[: 2 * n]
        w_refs = refs[2 * n : 2 * n + len(blocks)]
        held_refs = refs[2 * n + len(blocks) : 2 * n + len(blocks) + len(held)]
        store = refs[-1]
        here = lax.axis_index("tp")
        spot = lax.axis_index("sp")
        for (block, side, _), ref in zip(blocks, w_refs):
            row = (groups.index(block // 2) * 2 + ((spot ^ block) & 1)) * half

            def action(row=row, ref=ref):
                store[pl.ds(pl.multiple_of(row, half), half), :] = ref[...]

            choose(side, action)

        if earlier is None:
            outs = refs[-len(groups) - 2 : -2]
            sums = refs[-2]
        else:
            outs = refs[-n - 3 : -3]
            last, sums = refs[-3:-1]
        for i in range(tiles):
            rows = slice(i * WINDOW, (i + 1) * WINDOW)
            mix = mixed_tile(i, tok_rows, masks, hidden_refs, store)
            total, square = folded(mix), folded(mix * mix)
            whole = mix.astype(jnp.bfloat16)
            if earlier is None:
                sums[8 * i : 8 * i + 1, :] = total
                sums[8 * i + 1 : 8 * i + 2, :] = square
                for k, out in enumerate(outs):
                    out[rows, :] = whole[:, k * share : (k + 1) * share]
            else:
                last[rows, :] = whole
                sums[8 * i : 8 * (i + 1), :] = three_terms(
                    total + held_refs[-1][8 * i : 8 * i + 1, :],
                    square + held_refs[-1][8 * i + 1 : 8 * i + 2, :],
                )
        if earlier is None:
            return
        sources = [*held_refs[:-1], last]
        for mask, out in zip(masks, outs):
            out[tok_rows:, :] = sums[...].astype(jnp.bfloat16)
            distance = (spot >> 1) ^ here ^ mask
            for k, source in enumerate(sources):
                @pl.when(distance == k)
                def _():
                    out[0:tok_rows, :] = source[...]

    store = pltpu.VMEM((cols, depth * n), jnp.bfloat16)
    if earlier is None:
        outs = [shape((tok_rows, share)) for _ in groups]
        outs.append(shape((8 * tiles, WINDOW), jnp.float32))
        scratch = [store]
    else:
        outs = [shape((tok_rows + 8 * tiles, share)) for _ in masks]
        scratch = [
            pltpu.VMEM((tok_rows, share), jnp.bfloat16),
            pltpu.VMEM((8 * tiles, WINDOW), jnp.float32),
            store,
        ]
    return call(
        body,
        [*inner.values(), *outer.values()] + [part for *_, part in blocks] + held,
        outs,
        scratch,
        2 * tok_rows * depth * n * cols,
    )


def mix_staged(inner, outer, weights, tok_rows):
    pairs = len(weights) // 2
    early = mix_step(inner, outer, weights, tok_rows, list(range(pairs - 1)))
    late = mix_step(inner, outer, weights, tok_rows, [pairs - 1], early)
    return dict(zip(inner, late))


def close(pieces, out_gain, tok_rows, slice_cols):
    masks = list(pieces)
    held, share = pieces[0].shape
    width = out_gain.shape[0]
    model_width = width * len(masks)
    tile = min(TILE, tok_rows)

    def moments(sums):
        mean = sum(sums[k : k + 1] for k in range(3)) / model_width
        square = sum(sums[k : k + 1] for k in range(3, 6)) / model_width
        return mean, lax.rsqrt(square - mean * mean + epsilon)

    if slice_cols % 64:
        here = lax.axis_index("tp")
        stacked = jnp.zeros((len(masks), held, share), jnp.bfloat16)
        for mask, part in pieces.items():
            stacked = lax.dynamic_update_slice_in_dim(stacked, part[None], here ^ mask, 0)
        sums = jnp.sum(stacked[:, tok_rows:].astype(jnp.float32), axis=0)
        mean, scale = moments(sums.reshape(-1, 8, tile).transpose(1, 0, 2).reshape(8, -1))
        grid = stacked[:, :tok_rows].reshape(len(masks), tok_rows, -1, slice_cols)
        mixed = grid.transpose(1, 2, 0, 3).reshape(tok_rows, width).astype(jnp.float32)
        return ((mixed - mean.T) * scale.T * out_gain).astype(jnp.bfloat16)

    def body(*refs):
        n = len(masks)
        piece_refs = refs[:n]
        gain_ref, out_ref, store = refs[n:]
        here = lax.axis_index("tp")
        total = None
        for mask, ref in zip(masks, piece_refs):
            store[here ^ mask] = ref[0:tok_rows, :]
            sums = ref[tok_rows:, :].astype(jnp.float32)
            total = sums if total is None else total + sums
        for i in range(tok_rows // tile):
            rows = slice(i * tile, (i + 1) * tile)
            mean, scale = moments(total[8 * i : 8 * (i + 1)])
            mean = jnp.broadcast_to(mean, (128, tile)).T[:, 0:1]
            scale = jnp.broadcast_to(scale, (128, tile)).T[:, 0:1]
            parts = []
            for block in range(share // slice_cols):
                cols = slice(block * slice_cols, (block + 1) * slice_cols)
                parts += [store[k, rows, cols] for k in range(n)]
            mixed = jnp.concatenate(parts, axis=1).astype(jnp.float32)
            out_ref[rows, :] = ((mixed - mean) * scale * gain_ref[...]).astype(jnp.bfloat16)

    return call(
        body,
        [pieces[m] for m in masks] + [out_gain.reshape(1, width)],
        shape((tok_rows, width)),
        [pltpu.VMEM((len(masks), tok_rows, share), jnp.bfloat16)],
        8 * tok_rows * width,
    )


def local(
    tokens,
    w_query,
    w_key,
    w_value,
    w_pool_in,
    sink,
    w_pool,
    pool_scale,
    w_out_attn,
    w_out_pool,
    out_gain,
):
    tok_rows = tokens.shape[0]
    tp_count = lax.axis_size("tp")
    seq_len = tok_rows * lax.axis_size("sp")
    key_cols = w_key.shape[1]

    joined = pack_in(w_query, w_key, w_value, w_pool_in)
    weights = gather_sp(joined)
    all_tokens = gather_tp(tokens)

    turned = pack_out(w_out_attn, w_out_pool, tp_count)
    slice_cols, _ = turned[0].shape
    parts = [turned[0]] + [swap(turned[mask], "tp", mask) for mask in range(1, tp_count)]
    others = [sink.reshape(1, -1), pool_scale.reshape(1, -1), tokens]
    mine, sink, pool_scale, all_tokens[0] = assemble(parts, others)
    out_weights = gather_sp(mine, True)

    rim = 2 ** (POOL_GROUPS - 1)
    widths = [2 * key_cols, w_query.shape[1], w_pool_in.shape[1]]
    staged = len(weights) == 2 * tp_count
    step = project_staged if staged else project
    key_value, query, chan, near, far = step(all_tokens, weights, widths, rim)
    halo = exchange(near, far)
    small = (sink, w_pool, pool_scale, key_cols, seq_len)
    inner = gather_tp(hidden_inner(query, key_value, chan, *small))
    outer = gather_tp(hidden_outer(query, key_value, chan, halo, *small))
    mix = mix_staged if staged else mix_out
    pieces = mix(inner, outer, out_weights, tok_rows)
    pieces = {m: p if m == 0 else swap(p, "tp", m) for m, p in pieces.items()}
    return close(pieces, out_gain, tok_rows, slice_cols)


def solution(mesh):
    return jax.shard_map(
        local,
        mesh=mesh,
        in_specs=(
            P("sp", "tp"),
            P("sp", "tp"),
            P("sp", "tp"),
            P("sp", "tp"),
            P("sp", "tp"),
            P("tp"),
            P("tp", None, None),
            P("tp"),
            P("tp", "sp"),
            P("tp", "sp"),
            P("tp"),
        ),
        out_specs=P("sp", "tp"),
        check_vma=False,
    )
```
